256 devices in a mesh: grp: 2 (over y), sp: 32 (over z, core), tp: 4 (over x).
Axes of the slice: x: 4, y: 2, z: 16, core: 2. Of those that a mesh axis runs over, the one named last changes fastest.
The devices are a block of a 4x16x16 slice.
Arguments:
- receptance: bfloat16 [8192, 1024], P(('grp', 'sp'), 'tp'), parts along dimension 0, may hold values from -6 to 6
- head_keys: bfloat16 [8192, 1024], P(('grp', 'sp'), 'tp'), parts along dimension 0, may hold values from -6 to 6
- head_values: bfloat16 [8192, 1024], P(('grp', 'sp'), 'tp'), parts along dimension 0, may hold values from -6 to 6
- decay_logits: bfloat16 [8192, 1024], P(('grp', 'sp'), 'tp'), parts along dimension 0, may hold values from -13 to 0
- decay_boost: float32 [8192, 1024], P(('grp', 'sp'), 'tp'), parts along dimension 0, may hold values from -1.4 to 0
- correction_logits: bfloat16 [8192, 1024], P(('grp', 'sp'), 'tp'), parts along dimension 0, may hold values from -6 to 4
- gate_logits: bfloat16 [8192, 1024], P(('grp', 'sp'), 'tp'), parts along dimension 0, may hold values from -8 to 8
- head_norm_gain: float32 [1024], P('tp'), may hold values from 0.1 to 1.9
- output_weight: bfloat16 [1024, 2048], P('tp'), may hold values from -0.1875 to 0.1875
- residual: bfloat16 [8192, 2048], P(('grp', 'sp', 'tp')), parts along dimension 0, may hold values from -4 to 4
- expert_norm_gain: float32 [2048], replicated, may hold values from 0.1 to 1.9
- routes: int32 [8192, 2], P(('grp', 'sp', 'tp')), parts along dimension 0, may hold values from 0 to 31, all different within a row; in each aligned block of 32 rows (0 to 31, 32 to 63, ...) at most 4 rows name the same one
- routing_weight: float32 [8192, 2], P(('grp', 'sp', 'tp')), parts along dimension 0, may hold values from 0.1 to 1
- expert_gate_weight: bfloat16 [32, 2048, 3584], P('sp', None, 'tp'), may hold values from -0.125 to 0.125
- expert_up_weight: bfloat16 [32, 2048, 3584], P('sp', None, 'tp'), may hold values from -0.125 to 0.125
- expert_down_weight: bfloat16 [32, 3584, 2048], P('sp', 'tp'), may hold values from -0.09375 to 0.09375
Outputs:
- layer_out: bfloat16 [8192, 2048], P(('grp', 'sp', 'tp')), parts along dimension 0
The draws below stay inside these ranges and needn't reach their ends.
There are 2 independent parts, one for each index of `grp`. The reference program is written for one: setup_inputs(seed, part) draws one part's arguments, and reference() takes and returns one part's arrays. A program takes and returns all parts, laid end to end along the dimension named above; an argument that names none is the same for every part. Nothing has to cross between parts.
Inputs may be any that keep to these rules, and one draw needn't show every extreme that they name: Each row names 2 different experts. Among the positions that one index of sp+tp holds in routes, no expert is named by more than 4 of them, and in every draw some expert is named by exactly 4 of them there.
All inputs are finite; a program needn't handle non-finite values.
Results may differ from the reference program's by a relative error of at most 0.017.
Values may be sent and summed in bfloat16 or wider, within the bound.
No kernel may reach another device: no remote copies, remote signals or barrier semaphores. Data moves between devices by JAX's collectives and lax.ppermute only.
A program may use at most 64 MiB of HBM per device.

```python
import math
import jax
import jax.numpy as jnp
import numpy as np
from jax import lax

D = 2048
HEADS = 16
HEAD = 64
FF = 3584
TOP = 2
TOK_DEV = 128
TOKENS = 4096
HW = 1024
HEADS_DEV = 4
FF_DEV = 896
EXPERTS = 32
CAP = 4
N_SP = 32
N_TP = 4


def head_speed(key):
    order = jax.random.permutation(jax.random.fold_in(key, 101), HEADS)
    return order < HEADS // 2


def draw_decay_logits(key, part):
    quick = head_speed(key)
    fast_level = jax.random.uniform(jax.random.fold_in(key, 1), (HEADS,), jnp.float32, -3.8, -2.6)
    slow_level = jax.random.uniform(jax.random.fold_in(key, 2), (HEADS,), jnp.float32, -10.0, -8.5)
    offset = jnp.where(quick, fast_level, slow_level)
    stretch = jax.random.uniform(jax.random.fold_in(key, 3), (TOKENS // TOK_DEV, HEADS), jnp.float32, -0.7, 0.7)
    stretch = jnp.repeat(stretch, TOK_DEV, axis=0)
    jitter = jnp.clip(0.6 * jax.random.normal(jax.random.fold_in(key, 4), (TOKENS, HEADS, HEAD), jnp.float32), -1.8, 1.8)
    values = offset[None, :, None] + stretch[:, :, None] + jitter
    return values.reshape(TOKENS, HEADS * HEAD).astype(jnp.bfloat16)


def draw_correction_logits(key, part):
    quick = head_speed(key)
    fast_level = jax.random.uniform(jax.random.fold_in(key, 11), (HEADS,), jnp.float32, -1.0, 1.0)
    slow_level = jax.random.uniform(jax.random.fold_in(key, 12), (HEADS,), jnp.float32, -3.0, -2.0)
    offset = jnp.where(quick, fast_level, slow_level)
    jitter = jnp.clip(0.7 * jax.random.normal(jax.random.fold_in(key, 13), (TOKENS, HEADS, HEAD), jnp.float32), -2.1, 2.1)
    values = offset[None, :, None] + jitter
    return values.reshape(TOKENS, HEADS * HEAD).astype(jnp.bfloat16)


def draw_decay_boost(key, part):
    places = jax.random.randint(jax.random.fold_in(key, 21), (2, HEADS), 0, TOKENS)
    depth = jnp.log(jax.random.uniform(jax.random.fold_in(key, 22), (2, HEADS, HEAD), jnp.float32, 0.5, 0.8))
    position = jnp.arange(TOKENS)[:, None]
    total = jnp.zeros((TOKENS, HEADS, HEAD), jnp.float32)
    for turn in range(2):
        struck = (position == places[turn][None, :]).astype(jnp.float32)
        total = total + struck[:, :, None] * depth[turn][None, :, :]
    return total.reshape(TOKENS, HEADS * HEAD)


def block_scale(stream_key, dims, cuts, least, largest):
    level, own = 1.0, jax.random.fold_in(stream_key, 6)
    for dim, parts in cuts:
        heights = jnp.exp(jax.random.uniform(jax.random.fold_in(own, dim), (parts,), jnp.float32, least / len(cuts), largest / len(cuts)))
        level = level * jnp.repeat(heights, dims[dim] // parts).reshape([-1 if axis == dim else 1 for axis in range(len(dims))])
    return level


def assign_block(key, own, number, rows, amount, top, limit, skew):
    ranking = jax.random.permutation(key, amount)
    packed, ordinary = load_shares(amount, rows * top, limit, skew, True), load_shares(amount, rows * top, limit, skew, False)
    places = jnp.arange(amount)

    def named(tallies, turn):
        used = int((tallies > 0).sum())
        fixed = max(1, used // 4)
        moved = fixed + (places - fixed + turn * (used - fixed)) % max(1, amount - fixed)
        return jnp.zeros((amount,), jnp.int32).at[ranking[jnp.where(places < fixed, places, moved)]].set(jnp.asarray(tallies, jnp.int32))

    tallies = jnp.where(number % 4 == 0, named(packed, number // 4), named(ordinary, number - number // 4 - 1))
    mixed = jax.random.permutation(jax.random.fold_in(own, 3), amount)
    donor, taker = mixed[0:amount // 2 * 2:2], mixed[1:amount // 2 * 2:2]
    room = jnp.minimum(tallies[donor] - 1, limit - tallies[taker]) // 2
    room = jnp.where((donor == ranking[0]) | (taker == ranking[0]) | (tallies[taker] == 0), 0, jnp.maximum(room, 0))
    moved = jax.random.randint(jax.random.fold_in(own, 4), (amount // 2,), 0, 1 << 20) % (room + 1)
    tallies = tallies.at[donor].add(-moved).at[taker].add(moved)
    items = jnp.searchsorted(jnp.cumsum(tallies), jnp.arange(rows * top), side="right").astype(jnp.int32)
    table = items.reshape(top, rows).T
    table = table[jax.random.permutation(jax.random.fold_in(own, 1), rows)]
    turn = jax.random.randint(jax.random.fold_in(own, 2), (rows, 1), 0, top)
    return jnp.take_along_axis(table, (jnp.arange(top)[None, :] + turn) % top, axis=1)


def load_shares(amount, total, limit, slope, full):
    loads = [(1 << 20) // math.isqrt(grade ** slope) + 1 for grade in range(1, amount + 1)]
    largest = limit if full else min(limit, max(-(-total // amount), total * loads[0] // sum(loads)))
    least = 1 if total - largest >= amount - 1 else 0
    given, rest = [largest] + [least] * (amount - 1), total - largest - least * (amount - 1)
    while rest > 0:
        free = [i for i in range(1, amount) if given[i] < largest] or [i for i in range(1, amount) if given[i] < limit]
        mass, left = sum([loads[i] for i in free]), rest
        for i in free:
            extra = min(limit - given[i], max(1, left * loads[i] // mass), rest)
            given[i] = given[i] + extra
            rest = rest - extra
    return np.array(given)


def normal_values(own_key, shape, scale, limit, pieces=(), kind=jnp.bfloat16):
    loudness = block_scale(own_key, shape, pieces, -0.22, 0.18) if pieces else 1.0
    values = jax.random.normal(own_key, shape, jnp.float32) * scale * loudness
    return jnp.minimum(jnp.maximum(values, -limit), limit).astype(kind)


def setup_inputs(seed: int = 0, part: int = 0) -> dict:
    arg_keys = jax.random.split(jax.random.key(seed), 17)
    part_keys = jax.random.split(jax.random.fold_in(arg_keys[16], part), 17)
    receptance = normal_values(part_keys[0], (TOKENS, HW), 1.0, 6.0, ((0, 32), (1, 4)))
    head_keys = normal_values(part_keys[1], (TOKENS, HW), 1.0, 6.0, ((0, 32), (1, 4)))
    head_values = normal_values(part_keys[2], (TOKENS, HW), 1.0, 6.0, ((0, 32), (1, 4)))
    decay_logits = draw_decay_logits(jax.random.fold_in(jax.random.fold_in(arg_keys[16], part), 71), part)
    decay_boost = draw_decay_boost(jax.random.fold_in(jax.random.fold_in(arg_keys[16], part), 71), part)
    correction_logits = draw_correction_logits(jax.random.fold_in(jax.random.fold_in(arg_keys[16], part), 71), part)
    gate_logits = normal_values(part_keys[6], (TOKENS, HW), 1.5, 8.0, ((0, 32), (1, 4)))
    head_norm_gain = jnp.clip(1.0 + 0.18 * jax.random.normal(arg_keys[7], (HW,), jnp.float32), 0.1, 1.9)
    output_weight = normal_values(arg_keys[8], (HW, D), HW ** -0.5, 0.1875, ((0, 4),))
    residual = normal_values(part_keys[9], (TOKENS, D), 0.5, 4.0, ((0, 128),))
    expert_norm_gain = jnp.clip(1.0 + 0.18 * jax.random.normal(arg_keys[10], (D,), jnp.float32), 0.1, 1.9)
    routes_keys = jax.random.split(jax.random.fold_in(part_keys[11], 1), TOKENS // (TOK_DEV // N_TP))
    routes_turns = jax.random.permutation(jax.random.fold_in(part_keys[11], 3), TOKENS // (TOK_DEV // N_TP))
    routes = jax.vmap(lambda own, number: assign_block(jax.random.fold_in(part_keys[11], 2), own, number, TOK_DEV // N_TP, EXPERTS, TOP, CAP, 2))(routes_keys, routes_turns).reshape((TOKENS, TOP))
    routing_weight = jnp.clip(0.1 + 0.9 * jax.random.uniform(part_keys[12], (TOKENS, TOP), jnp.float32) ** block_scale(part_keys[12], (TOKENS, TOP), ((0, 128),), -0.2, 0.2), 0.1, 1.0)
    expert_gate_weight = normal_values(arg_keys[13], (EXPERTS, D, FF), D ** -0.5, 0.125, ((0, 32), (2, 4)))
    expert_up_weight = normal_values(arg_keys[14], (EXPERTS, D, FF), D ** -0.5, 0.125, ((0, 32), (2, 4)))
    expert_down_weight = normal_values(arg_keys[15], (EXPERTS, FF, D), FF ** -0.5, 0.09375, ((0, 32), (1, 4)))
    return {"receptance": receptance, "head_keys": head_keys, "head_values": head_values, "decay_logits": decay_logits, "decay_boost": decay_boost, "correction_logits": correction_logits, "gate_logits": gate_logits, "head_norm_gain": head_norm_gain, "output_weight": output_weight, "residual": residual, "expert_norm_gain": expert_norm_gain, "routes": routes, "routing_weight": routing_weight, "expert_gate_weight": expert_gate_weight, "expert_up_weight": expert_up_weight, "expert_down_weight": expert_down_weight}


highest = lax.Precision.HIGHEST

def heads_divide(array):
    return array.astype(jnp.float32).reshape(array.shape[0], HEADS, HEAD)

def recurrence(state, inputs):
    query, decay_factor, keyed, valued, remove, insert = inputs
    along = jnp.einsum('hvk,hk->hv', state, remove, precision=highest)
    state = state * decay_factor[:, None, :] + along[:, :, None] * insert[:, None, :] + valued[:, :, None] * keyed[:, None, :]
    return (state, jnp.einsum('hvk,hk->hv', state, query, precision=highest))

def reference(receptance, head_keys, head_values, decay_logits, decay_boost, correction_logits, gate_logits, head_norm_gain, output_weight, residual, expert_norm_gain, routes, routing_weight, expert_gate_weight, expert_up_weight, expert_down_weight):
    query = heads_divide(receptance)
    keyed = heads_divide(head_keys)
    valued = heads_divide(head_values)
    unit = keyed * lax.rsqrt(lax.optimization_barrier(jnp.sum(keyed * keyed, axis=-1, keepdims=True)) + 1e-06)
    rate = jax.nn.sigmoid(heads_divide(correction_logits))
    decay_factor = jnp.exp(-jnp.exp(-jax.nn.softplus(-heads_divide(decay_logits)) - 0.5) + heads_divide(decay_boost))
    start = jnp.zeros((HEADS, HEAD, HEAD), jnp.float32)
    _, mixed = lax.scan(recurrence, start, (query, decay_factor, keyed, valued, -unit, unit * rate))
    centre = mixed - lax.optimization_barrier(jnp.mean(mixed, axis=-1, keepdims=True))
    spread = lax.optimization_barrier(jnp.mean(centre * centre, axis=-1, keepdims=True))
    normed = centre * lax.rsqrt(spread + 0.00064) * head_norm_gain.reshape(HEADS, HEAD)
    gated = (normed.reshape(TOKENS, HW) * jax.nn.sigmoid(gate_logits.astype(jnp.float32))).astype(jnp.bfloat16)
    group = HEADS_DEV * HEAD
    branch = jnp.zeros((TOKENS, D), jnp.float32)
    for group_index in range(N_TP):
        lower = group_index * group
        piece = jnp.dot(gated[:, lower:lower + group], output_weight[lower:lower + group], preferred_element_type=jnp.float32).astype(jnp.bfloat16)
        piece = lax.optimization_barrier(piece)
        branch = branch + piece.astype(jnp.float32)
    stream = residual.astype(jnp.float32) + branch
    normal = (stream * lax.rsqrt(lax.optimization_barrier(jnp.mean(stream * stream, axis=-1, keepdims=True)) + 1e-06) * expert_norm_gain).astype(jnp.bfloat16)
    flat_routes = routes.reshape(-1).astype(jnp.int32)
    most_rows = CAP * N_SP * N_TP

    def per_expert(total, item):
        gate_w, up_w, down_w, expert_index = item
        chosen = flat_routes == expert_index
        order = jnp.argsort(jnp.where(chosen, 0, 1).astype(jnp.int32), stable=True)[:most_rows].astype(jnp.int32)
        live = chosen[order]
        rows = normal[order // TOP]
        hidden = (jax.nn.silu(jnp.dot(rows, gate_w, preferred_element_type=jnp.float32)) * jnp.dot(rows, up_w, preferred_element_type=jnp.float32)).astype(jnp.bfloat16)
        result = jnp.zeros((most_rows, D), jnp.float32)
        for slice_index in range(N_TP):
            lower = slice_index * FF_DEV
            piece = jnp.dot(hidden[:, lower:lower + FF_DEV], down_w[lower:lower + FF_DEV], preferred_element_type=jnp.float32).astype(jnp.bfloat16)
            piece = lax.optimization_barrier(piece)
            result = result + piece.astype(jnp.float32)
        result = lax.optimization_barrier(result.astype(jnp.bfloat16)).astype(jnp.float32)
        total = total.at[order].add(jnp.where(live[:, None], result, jnp.float32(0.0)))
        return (total, None)
    pairs, _ = lax.scan(per_expert, jnp.zeros((TOKENS * TOP, D), jnp.float32), (expert_gate_weight, expert_up_weight, expert_down_weight, jnp.arange(EXPERTS, dtype=jnp.int32)))
    routed = lax.optimization_barrier(jnp.sum(pairs.reshape(TOKENS, TOP, D) * routing_weight[:, :, None], axis=1))
    return (stream + routed).astype(jnp.bfloat16)
```

```python
import math

import jax
import jax.numpy as jnp
from jax import lax
from jax.experimental import pallas as pl
from jax.experimental.pallas import tpu as pltpu
from jax.sharding import Mesh
from jax.sharding import PartitionSpec as P

HEAD = 64
TOP = 2
BLK = 32
QUAD = 4
HALF_DOWN = math.exp(-0.5)
TOK_DEV = 128
SP = ("sp_0", "sp_1")
GRP_SP = ("grp", "sp_0", "sp_1")
GRP_SP_TP = ("grp", "sp_0", "sp_1", "tp")


highest = lax.Precision.HIGHEST


def shifted(x, axis, step):
    size = lax.axis_size(axis)
    return lax.ppermute(x, axis, [(i, (i + step) % size) for i in range(size)])


def within_quads(x, axis, step):
    size = lax.axis_size(axis)
    pairs = [(i, i // QUAD * QUAD + (i % QUAD + step) % QUAD) for i in range(size)]
    return lax.ppermute(x, axis, pairs)


def across_quads(x, axis, step):
    size = lax.axis_size(axis)
    return lax.ppermute(x, axis, [(i, i + step * QUAD) for i in range(size - step * QUAD)])


def after(later, earlier):
    moved = jnp.einsum("hij,hjk->hik", later[..., :HEAD], earlier, precision=highest)
    return moved + jnp.where(jnp.arange(2 * HEAD) < HEAD, 0.0, later)


def onto(later, state):
    moved = jnp.einsum("hij,hjk->hik", later[..., :HEAD], state, precision=highest)
    return moved + later[..., HEAD:]


def incoming_state(packed):
    wide = jnp.float32
    core = lax.axis_index("sp_1")
    own = packed.astype(wide)
    other = shifted(packed, "sp_1", 1).astype(wide)
    first = jnp.where(core == 0, own, other)
    second = jnp.where(core == 0, other, own)
    half = own.shape[0] // 2
    chip = after(
        lax.dynamic_slice_in_dim(second, core * half, half, 0),
        lax.dynamic_slice_in_dim(first, core * half, half, 0),
    )
    sent = chip.astype(jnp.bfloat16)
    member = lax.axis_index("sp_0") % QUAD
    came = [chip] + [within_quads(sent, "sp_0", k).astype(wide) for k in range(1, QUAD)]
    came = jnp.stack(came)
    total = lax.dynamic_index_in_dim(came, member % QUAD, 0, False)
    eye = jnp.eye(HEAD, 2 * HEAD, dtype=wide)
    before = jnp.where(member == 0, eye, total)
    for k in range(1, QUAD):
        piece = lax.dynamic_index_in_dim(came, (member - k) % QUAD, 0, False)
        total = after(piece, total)
        if k < QUAD - 1:
            before = jnp.where(member == k + 1, total, before)
    sent = total.astype(jnp.bfloat16)
    far = [across_quads(sent, "sp_0", k).astype(wide) for k in range(QUAD - 1, 0, -1)]
    reach = far[0][..., HEAD:]
    for piece in far[1:]:
        reach = onto(piece, reach)
    reach = onto(before, reach)
    mine = jnp.concatenate([reach[0], reach[1]], axis=1)
    swapped = shifted(mine.astype(jnp.bfloat16), "sp_1", 1).astype(wide)
    low = jnp.where(core == 0, mine, swapped)
    high = jnp.where(core == 0, swapped, mine)
    every = jnp.stack([low[:, :HEAD], low[:, HEAD:], high[:, :HEAD], high[:, HEAD:]])
    return other.astype(jnp.bfloat16), every


def gathered_weight(weight):
    half = weight.shape[1] // 2
    core = lax.axis_index("sp_1")
    mine = lax.dynamic_slice_in_dim(weight, core * half, half, 1)
    parts = [mine] + [shifted(mine, "tp", k) for k in (1, 3, 2)]
    mine = jnp.concatenate(parts, axis=0)
    other = shifted(mine, "sp_1", 1)
    return jnp.concatenate([jnp.where(core == 0, mine, other), jnp.where(core == 0, other, mine)], axis=1)


def own_rows(rows):
    count = lax.axis_size("tp")
    mine = lax.axis_index("tp")
    blocks = rows.reshape(count, -1, rows.shape[1])
    parts = [lax.dynamic_index_in_dim(blocks, mine, 0, False)]
    for k in (1, 3, 2):
        block = lax.dynamic_index_in_dim(blocks, (mine + k) % count, 0, False)
        parts.append(shifted(block, "tp", k))
    return jnp.concatenate(parts, axis=1)


def split_dot(first, second):
    high_a, high_b = first.astype(jnp.bfloat16), second.astype(jnp.bfloat16)
    low_a = (first - high_a.astype(jnp.float32)).astype(jnp.bfloat16)
    low_b = (second - high_b.astype(jnp.float32)).astype(jnp.bfloat16)
    return plain_dot(high_a, high_b) + (plain_dot(high_a, low_b) + plain_dot(low_a, high_b))


def plain_dot(first, second, dims=((1,), (0,))):
    return lax.dot_general(
        first.astype(jnp.bfloat16),
        second.astype(jnp.bfloat16),
        (dims, ((), ())),
        preferred_element_type=jnp.float32,
    )


def scan_kernel(query_ref, key_ref, value_ref, decay_ref, boost_ref, rate_ref, out_ref, whole_ref):
    wide, narrow = jnp.float32, jnp.bfloat16
    length, width = key_ref.shape
    heads = width // HEAD
    blocks = length // BLK
    keyed = key_ref[...].astype(wide)
    query = query_ref[...].astype(wide)
    valued = value_ref[...]
    lane_r = lax.broadcasted_iota(jnp.int32, (width, width), 0) // HEAD
    lane_c = lax.broadcasted_iota(jnp.int32, (width, width), 1) // HEAD
    same_head = (lane_r == lane_c).astype(narrow)
    square = keyed * keyed
    square_high = square.astype(narrow)
    square_low = (square - square_high.astype(wide)).astype(narrow)
    norm = plain_dot(square_high, same_head) + plain_dot(square_low, same_head)
    unit = keyed * lax.rsqrt(norm + 1e-06)
    insert = unit * jax.nn.sigmoid(rate_ref[...].astype(wide))
    slow = jax.nn.sigmoid(decay_ref[...].astype(wide)) * HALF_DOWN
    log_decay = boost_ref[...] - slow
    row = lax.broadcasted_iota(jnp.int32, (length, length), 0)
    col = lax.broadcasted_iota(jnp.int32, (length, length), 1)
    same_block = row // BLK == col // BLK
    strict = same_block & (row > col)
    inclusive = same_block & (row >= col)
    sums = jnp.concatenate([inclusive.astype(narrow), same_block.astype(narrow)], axis=0)
    part, added = log_decay, 0.0
    for _ in range(3):
        piece = part.astype(narrow)
        added = added + plain_dot(sums, piece)
        part = part - piece.astype(wide)
    upto, final = added[:length], added[length:]
    remove_scaled = -unit * jnp.exp(upto - log_decay)
    query_scaled = query * jnp.exp(upto)
    shrink = jnp.exp(-upto)
    insert_scaled = (insert * shrink).astype(narrow)
    key_scaled = (keyed * shrink).astype(narrow)
    tail = jnp.exp(final - upto)
    insert_tail = (insert * tail).astype(narrow)
    key_tail = (keyed * tail).astype(narrow)
    kept = jnp.exp(final)
    every = range(heads)
    lanes = [slice(h * HEAD, (h + 1) * HEAD) for h in every]
    pair = [
        plain_dot(
            jnp.concatenate([remove_scaled[:, lanes[h]], query_scaled[:, lanes[h]]], axis=0),
            jnp.concatenate([insert_scaled[:, lanes[h]], key_scaled[:, lanes[h]]], axis=0),
            ((1,), (1,)),
        )
        for h in every
    ]
    among = [jnp.where(strict, pair[h][:length, :length], 0.0).astype(narrow) for h in every]
    read = [jnp.where(inclusive, pair[h][length:, :length], 0.0).astype(narrow) for h in every]
    by_keys = [
        jnp.concatenate(
            [
                jnp.where(strict, pair[h][:length, length:], 0.0),
                jnp.where(inclusive, pair[h][length:, length:], 0.0),
            ],
            axis=0,
        ).astype(narrow)
        for h in every
    ]
    from_values = [plain_dot(by_keys[h], valued[:, lanes[h]]) for h in every]
    solved = [
        jnp.concatenate([remove_scaled[:, lanes[h]], from_values[h][:length]], axis=1)
        for h in every
    ]
    power = among
    covered = 1
    while covered < BLK:
        solved = [solved[h] + plain_dot(power[h], solved[h]) for h in every]
        covered = 2 * covered
        if covered < BLK:
            power = [plain_dot(power[h], power[h]).astype(narrow) for h in every]
    reading = [
        jnp.concatenate([query_scaled[:, lanes[h]], from_values[h][length:]], axis=1)
        + plain_dot(read[h], solved[h])
        for h in every
    ]
    wide_r = lax.broadcasted_iota(jnp.int32, (HEAD, 2 * HEAD), 0)
    wide_c = lax.broadcasted_iota(jnp.int32, (HEAD, 2 * HEAD), 1)
    diagonal = wide_r == wide_c
    is_state = wide_c >= HEAD
    none = jnp.zeros((BLK, HEAD), narrow)
    so_far = [None] * heads
    for n in range(blocks):
        rows = slice(n * BLK, (n + 1) * BLK)
        maps = []
        for h in every:
            sources = jnp.concatenate([insert_tail[rows, lanes[h]], key_tail[rows, lanes[h]]], axis=0)
            targets = jnp.concatenate(
                [
                    solved[h][rows].astype(narrow),
                    jnp.concatenate([none, valued[rows, lanes[h]]], axis=1),
                ],
                axis=0,
            )
            keeps = kept[n * BLK : n * BLK + 1, lanes[h]]
            keeps = jnp.concatenate([keeps, keeps], axis=1)
            maps.append(
                plain_dot(sources, targets, ((0,), (0,))) + jnp.where(diagonal, keeps, 0.0)
            )
        for h in every:
            here = reading[h][rows]
            if n == 0:
                out_ref[h, rows, :] = here
                so_far[h] = maps[h]
            else:
                moved = split_dot(here[:, :HEAD], so_far[h])
                local = lax.broadcasted_iota(jnp.int32, here.shape, 1) >= HEAD
                out_ref[h, rows, :] = moved + jnp.where(local, here, 0.0)
                so_far[h] = split_dot(maps[h][:, :HEAD], so_far[h]) + jnp.where(
                    is_state, maps[h], 0.0
                )
    for h in every:
        whole_ref[h] = so_far[h].astype(narrow)


def in_vmem(count):
    return [pl.BlockSpec(memory_space=pltpu.VMEM)] * count


def scanned(*arrays):
    length, width = arrays[0].shape
    heads = width // HEAD
    return pl.pallas_call(
        scan_kernel,
        out_shape=(
            jax.ShapeDtypeStruct((heads, length, 2 * HEAD), jnp.float32),
            jax.ShapeDtypeStruct((heads, HEAD, 2 * HEAD), jnp.bfloat16),
        ),
        in_specs=in_vmem(6),
        out_specs=tuple(in_vmem(2)),
        cost_estimate=pl.CostEstimate(flops=4_000_000_000, bytes_accessed=1 << 20, transcendentals=0),
        name="scan_blocks",
    )(*arrays)


def finish_kernel(core_ref, out_ref, first_ref, reach_ref, gate_ref, gain_ref, gated_ref):
    wide = jnp.float32
    heads = out_ref.shape[0]
    later_core = core_ref[0] > 0
    parts = []
    for h in range(heads):
        before = first_ref[h].astype(wide)
        reach = reach_ref[h]
        passed = split_dot(before[:, :HEAD], reach) + before[:, HEAD:]
        reach = jnp.where(later_core, passed, reach)
        here = out_ref[h]
        mixed = split_dot(here[:, :HEAD], reach) + here[:, HEAD:]
        centre = mixed - jnp.mean(mixed, axis=1, keepdims=True)
        spread = jnp.mean(centre * centre, axis=1, keepdims=True)
        parts.append(centre * lax.rsqrt(spread + 0.00064))
    normed = jnp.concatenate(parts, axis=1) * gain_ref[...]
    gated_ref[...] = (normed * jax.nn.sigmoid(gate_ref[...].astype(wide))).astype(gated_ref.dtype)


def finished(outputs, first, reach, gate_logits, gain):
    core = lax.axis_index("sp_1").astype(jnp.int32).reshape(1)
    return pl.pallas_call(
        finish_kernel,
        out_shape=jax.ShapeDtypeStruct(gate_logits.shape, jnp.bfloat16),
        in_specs=[pl.BlockSpec(memory_space=pltpu.SMEM), *in_vmem(5)],
        out_specs=in_vmem(1)[0],
        cost_estimate=pl.CostEstimate(flops=400_000_000, bytes_accessed=1 << 19, transcendentals=0),
        name="finish_heads",
    )(core, outputs, first, reach, gate_logits, gain.reshape(1, -1))


def body(
    receptance,
    head_keys,
    head_values,
    decay_logits,
    decay_boost,
    correction_logits,
    gate_logits,
    head_norm_gain,
    output_weight,
    residual,
    expert_norm_gain,
    routes,
    routing_weight,
    expert_gate_weight,
    expert_up_weight,
    expert_down_weight,
):
    with jax.named_scope("weight_x"):
        weight_here = gathered_weight(output_weight)
    outputs, whole = scanned(
        receptance, head_keys, head_values, decay_logits, decay_boost, correction_logits
    )
    first, reach = incoming_state(whole)
    gated = finished(outputs, first, reach, gate_logits, head_norm_gain)
    with jax.named_scope("rows_x"):
        rows_here = own_rows(gated)
    branch = jnp.dot(rows_here, weight_here, preferred_element_type=jnp.float32)
    stream = residual.astype(jnp.float32) + branch
    normal = (
        stream
        * lax.rsqrt(jnp.mean(stream * stream, axis=-1, keepdims=True) + 1e-06)
        * expert_norm_gain
    ).astype(jnp.bfloat16)
    sp_count = lax.axis_size(SP)
    tp_count = lax.axis_size("tp")
    z_count = lax.axis_size("sp_0")
    capacity = max(2, 2 * TOK_DEV * TOP // (tp_count * sp_count))
    local_count = normal.shape[0]
    width_model = normal.shape[1]
    core = lax.axis_index("sp_1")
    flat_routes = routes.reshape(-1)
    expert_ids = jnp.arange(sp_count, dtype=jnp.int32)
    chosen = (flat_routes[:, None] == expert_ids[None, :]).astype(jnp.int32)
    earlier = jnp.cumsum(chosen, axis=0) - chosen
    rank = jnp.sum(earlier * chosen, axis=1)
    away = jnp.where(flat_routes % 2 == core, 0, 1)
    place = (away * z_count + flat_routes // 2) * capacity + rank
    places = jnp.arange(sp_count * capacity, dtype=jnp.int32)
    onehot = (place[:, None] == places[None, :]).astype(jnp.bfloat16)
    placed = jnp.sum(onehot.reshape(local_count, TOP, sp_count * capacity), axis=1)
    placed, onehot, routing_weight = lax.optimization_barrier((placed, onehot, routing_weight))
    outbound = jnp.einsum("ts,td->sd", placed, normal, preferred_element_type=jnp.float32).astype(
        jnp.bfloat16
    )
    outbound = outbound.reshape(2, z_count, capacity, width_model)
    with jax.named_scope("out_core"):
        across = shifted(outbound[1], "sp_1", 1)
    going = jnp.concatenate([outbound[0], across], axis=1)
    with jax.named_scope("out_z"):
        arrived = lax.all_to_all(going, "sp_0", split_axis=0, concat_axis=0, tiled=True)
    arrived = arrived.reshape(-1, width_model)
    came = []
    for source, rows in enumerate([arrived] + [shifted(arrived, "tp", k) for k in (1, 3, 2)]):
        hidden = (
            jax.nn.silu(jnp.dot(rows, expert_gate_weight[0], preferred_element_type=jnp.float32))
            * jnp.dot(rows, expert_up_weight[0], preferred_element_type=jnp.float32)
        ).astype(jnp.bfloat16)
        partial_rows = jnp.dot(
            hidden, expert_down_weight[0], preferred_element_type=jnp.float32
        ).astype(jnp.bfloat16)
        came.append(shifted(partial_rows, "tp", -(0, 1, 3, 2)[source]) if source else partial_rows)
    total = sum(piece.astype(jnp.float32) for piece in came).astype(jnp.bfloat16)
    total = total.reshape(z_count, 2 * capacity, width_model)
    with jax.named_scope("back_z"):
        home = lax.all_to_all(total, "sp_0", split_axis=0, concat_axis=0, tiled=True)
    with jax.named_scope("back_core"):
        across = shifted(home[:, capacity:], "sp_1", 1)
    onehot = onehot.reshape(local_count * TOP, 2, z_count * capacity)
    picked = jnp.zeros((local_count * TOP, width_model), jnp.float32)
    for side, part in enumerate((home[:, :capacity], across)):
        picked = picked + jnp.dot(
            onehot[:, side], part.reshape(-1, width_model), preferred_element_type=jnp.float32
        )
    routed = jnp.sum(
        picked.reshape(local_count, TOP, width_model) * routing_weight[:, :, None], axis=1
    )
    return (stream + routed).astype(jnp.bfloat16)


def solution(mesh):
    torus = Mesh(
        mesh.devices.reshape(mesh.shape["grp"], 16, 2, mesh.shape["tp"]),
        ("grp", "sp_0", "sp_1", "tp"),
    )
    return jax.shard_map(
        body,
        mesh=torus,
        in_specs=(
            P(GRP_SP, "tp"),
            P(GRP_SP, "tp"),
            P(GRP_SP, "tp"),
            P(GRP_SP, "tp"),
            P(GRP_SP, "tp"),
            P(GRP_SP, "tp"),
            P(GRP_SP, "tp"),
            P("tp"),
            P("tp", None),
            P(GRP_SP_TP, None),
            P(),
            P(GRP_SP_TP, None),
            P(GRP_SP_TP, None),
            P(SP, None, "tp"),
            P(SP, None, "tp"),
            P(SP, "tp", None),
        ),
        out_specs=P(GRP_SP_TP, None),
        check_vma=False,
    )
```

```python
import math
from functools import partial

import jax
import jax.numpy as jnp
from jax import lax
from jax.experimental import pallas as pl
from jax.experimental.pallas import tpu as pltpu
from jax.sharding import Mesh
from jax.sharding import PartitionSpec as P


HEAD = 64
TOP = 2
BLK = 32
QUAD = 4
OFFSETS = (1, 3, 2)
FF_TILE = 256
LIMIT_FIRST = 42
LIMIT_REST = 18
HALF_DOWN = math.exp(-0.5)
TOK_DEV = 128
SP = ("sp_0", "sp_1")
GRP_SP = ("grp", "sp_0", "sp_1")
GRP_SP_TP = ("grp", "sp_0", "sp_1", "tp")


highest = lax.Precision.HIGHEST


def shifted(x, axis, step):
    size = lax.axis_size(axis)
    return lax.ppermute(x, axis, [(i, (i + step) % size) for i in range(size)])


def within_quads(x, axis, step):
    size = lax.axis_size(axis)
    pairs = [(i, i // QUAD * QUAD + (i % QUAD + step) % QUAD) for i in range(size)]
    return lax.ppermute(x, axis, pairs)


def across_quads(x, axis, step):
    size = lax.axis_size(axis)
    return lax.ppermute(x, axis, [(i, i + step * QUAD) for i in range(size - step * QUAD)])


def after(later, earlier):
    moved = jnp.einsum("hij,hjk->hik", later[..., :HEAD], earlier, precision=highest)
    return moved + jnp.where(jnp.arange(2 * HEAD) < HEAD, 0.0, later)


def onto(later, state):
    moved = jnp.einsum("hij,hjk->hik", later[..., :HEAD], state, precision=highest)
    return moved + later[..., HEAD:]


def incoming_state(packed):
    wide = jnp.float32
    core = lax.axis_index("sp_1")
    own = packed.astype(wide)
    other = shifted(packed, "sp_1", 1).astype(wide)
    first = jnp.where(core == 0, own, other)
    second = jnp.where(core == 0, other, own)
    half = own.shape[0] // 2
    chip = after(
        lax.dynamic_slice_in_dim(second, core * half, half, 0),
        lax.dynamic_slice_in_dim(first, core * half, half, 0),
    )
    sent = chip.astype(jnp.bfloat16)
    member = lax.axis_index("sp_0") % QUAD
    came = [chip] + [within_quads(sent, "sp_0", k).astype(wide) for k in range(1, QUAD)]
    came = jnp.stack(came)
    total = lax.dynamic_index_in_dim(came, member % QUAD, 0, False)
    eye = jnp.eye(HEAD, 2 * HEAD, dtype=wide)
    before = jnp.where(member == 0, eye, total)
    for k in range(1, QUAD):
        piece = lax.dynamic_index_in_dim(came, (member - k) % QUAD, 0, False)
        total = after(piece, total)
        if k < QUAD - 1:
            before = jnp.where(member == k + 1, total, before)
    sent = total.astype(jnp.bfloat16)
    far = [across_quads(sent, "sp_0", k).astype(wide) for k in range(QUAD - 1, 0, -1)]
    reach = far[0][..., HEAD:]
    for piece in far[1:]:
        reach = onto(piece, reach)
    reach = onto(before, reach)
    mine = jnp.concatenate([reach[0], reach[1]], axis=1)
    swapped = shifted(mine.astype(jnp.bfloat16), "sp_1", 1).astype(wide)
    low = jnp.where(core == 0, mine, swapped)
    high = jnp.where(core == 0, swapped, mine)
    every = jnp.stack([low[:, :HEAD], low[:, HEAD:], high[:, :HEAD], high[:, HEAD:]])
    return other.astype(jnp.bfloat16), every


def gathered_weight(weight, behind):
    half = weight.shape[1] // 2
    core = lax.axis_index("sp_1")
    mine = lax.dynamic_slice_in_dim(weight, core * half, half, 1)
    partners = lax.dynamic_slice_in_dim(weight, (1 - core) * half, half, 1)
    mine, behind = lax.optimization_barrier((mine, behind))
    mine = [mine] + [shifted(mine, "tp", k) for k in OFFSETS]
    other = [partners] + [shifted(piece, "sp_1", 1) for piece in mine[1:]]
    return (mine, other), behind


def projected(rows, weights):
    core = lax.axis_index("sp_1")
    halves = [
        sum(jnp.dot(r, w, preferred_element_type=jnp.float32) for r, w in zip(rows, side))
        for side in weights
    ]
    mine, other = halves
    left, right = jnp.where(core == 0, mine, other), jnp.where(core == 0, other, mine)
    return jnp.concatenate([left, right], axis=1)


def own_rows(rows):
    count = lax.axis_size("tp")
    mine = lax.axis_index("tp")
    blocks = rows.reshape(count, -1, rows.shape[1])
    parts = [lax.dynamic_index_in_dim(blocks, mine, 0, False)]
    for k in OFFSETS:
        block = lax.dynamic_index_in_dim(blocks, (mine + k) % count, 0, False)
        parts.append(shifted(block, "tp", k))
    return parts


def split_dot(first, second):
    high_a, high_b = first.astype(jnp.bfloat16), second.astype(jnp.bfloat16)
    low_a = (first - high_a.astype(jnp.float32)).astype(jnp.bfloat16)
    low_b = (second - high_b.astype(jnp.float32)).astype(jnp.bfloat16)
    return plain_dot(high_a, high_b) + (plain_dot(high_a, low_b) + plain_dot(low_a, high_b))


def plain_dot(first, second, dims=((1,), (0,))):
    return lax.dot_general(
        first.astype(jnp.bfloat16),
        second.astype(jnp.bfloat16),
        (dims, ((), ())),
        preferred_element_type=jnp.float32,
    )


def scan_kernel(query_ref, key_ref, value_ref, decay_ref, boost_ref, rate_ref, out_ref, whole_ref):
    wide, narrow = jnp.float32, jnp.bfloat16
    length, width = key_ref.shape
    heads = width // HEAD
    blocks = length // BLK
    keyed = key_ref[...].astype(wide)
    query = query_ref[...].astype(wide)
    valued = value_ref[...]
    lane_r = lax.broadcasted_iota(jnp.int32, (width, width), 0) // HEAD
    lane_c = lax.broadcasted_iota(jnp.int32, (width, width), 1) // HEAD
    same_head = (lane_r == lane_c).astype(narrow)
    square = keyed * keyed
    square_high = square.astype(narrow)
    square_low = (square - square_high.astype(wide)).astype(narrow)
    norm = plain_dot(square_high, same_head) + plain_dot(square_low, same_head)
    unit = keyed * lax.rsqrt(norm + 1e-06)
    insert = unit * jax.nn.sigmoid(rate_ref[...].astype(wide))
    slow = jax.nn.sigmoid(decay_ref[...].astype(wide)) * HALF_DOWN
    log_decay = boost_ref[...] - slow
    row = lax.broadcasted_iota(jnp.int32, (length, length), 0)
    col = lax.broadcasted_iota(jnp.int32, (length, length), 1)
    same_block = row // BLK == col // BLK
    strict = same_block & (row > col)
    inclusive = same_block & (row >= col)
    sums = jnp.concatenate([inclusive.astype(narrow), same_block.astype(narrow)], axis=0)
    part, added = log_decay, 0.0
    for _ in range(3):
        piece = part.astype(narrow)
        added = added + plain_dot(sums, piece)
        part = part - piece.astype(wide)
    upto, final = added[:length], added[length:]
    remove_scaled = -unit * jnp.exp(upto - log_decay)
    query_scaled = query * jnp.exp(upto)
    shrink = jnp.exp(-upto)
    insert_scaled = (insert * shrink).astype(narrow)
    key_scaled = (keyed * shrink).astype(narrow)
    tail = jnp.exp(final - upto)
    insert_tail = (insert * tail).astype(narrow)
    key_tail = (keyed * tail).astype(narrow)
    kept = jnp.exp(final)
    every = range(heads)
    lanes = [slice(h * HEAD, (h + 1) * HEAD) for h in every]
    pair = [
        plain_dot(
            jnp.concatenate([remove_scaled[:, lanes[h]], query_scaled[:, lanes[h]]], axis=0),
            jnp.concatenate([insert_scaled[:, lanes[h]], key_scaled[:, lanes[h]]], axis=0),
            ((1,), (1,)),
        )
        for h in every
    ]
    among = [jnp.where(strict, pair[h][:length, :length], 0.0).astype(narrow) for h in every]
    read = [jnp.where(inclusive, pair[h][length:, :length], 0.0).astype(narrow) for h in every]
    by_keys = [
        jnp.concatenate(
            [
                jnp.where(strict, pair[h][:length, length:], 0.0),
                jnp.where(inclusive, pair[h][length:, length:], 0.0),
            ],
            axis=0,
        ).astype(narrow)
        for h in every
    ]
    from_values = [plain_dot(by_keys[h], valued[:, lanes[h]]) for h in every]
    solved = [
        jnp.concatenate([remove_scaled[:, lanes[h]], from_values[h][:length]], axis=1)
        for h in every
    ]
    power = among
    covered = 1
    while covered < BLK:
        solved = [solved[h] + plain_dot(power[h], solved[h]) for h in every]
        covered = 2 * covered
        if covered < BLK:
            power = [plain_dot(power[h], power[h]).astype(narrow) for h in every]
    reading = [
        jnp.concatenate([query_scaled[:, lanes[h]], from_values[h][length:]], axis=1)
        + plain_dot(read[h], solved[h])
        for h in every
    ]
    wide_r = lax.broadcasted_iota(jnp.int32, (HEAD, 2 * HEAD), 0)
    wide_c = lax.broadcasted_iota(jnp.int32, (HEAD, 2 * HEAD), 1)
    diagonal = wide_r == wide_c
    is_state = wide_c >= HEAD
    none = jnp.zeros((BLK, HEAD), narrow)
    so_far = [None] * heads
    for n in range(blocks):
        rows = slice(n * BLK, (n + 1) * BLK)
        maps = []
        for h in every:
            sources = jnp.concatenate([insert_tail[rows, lanes[h]], key_tail[rows, lanes[h]]], axis=0)
            targets = jnp.concatenate(
                [
                    solved[h][rows].astype(narrow),
                    jnp.concatenate([none, valued[rows, lanes[h]]], axis=1),
                ],
                axis=0,
            )
            keeps = kept[n * BLK : n * BLK + 1, lanes[h]]
            keeps = jnp.concatenate([keeps, keeps], axis=1)
            maps.append(
                plain_dot(sources, targets, ((0,), (0,))) + jnp.where(diagonal, keeps, 0.0)
            )
        for h in every:
            here = reading[h][rows]
            if n == 0:
                out_ref[h, rows, :] = here
                so_far[h] = maps[h]
            else:
                moved = split_dot(here[:, :HEAD], so_far[h])
                local = lax.broadcasted_iota(jnp.int32, here.shape, 1) >= HEAD
                out_ref[h, rows, :] = moved + jnp.where(local, here, 0.0)
                so_far[h] = split_dot(maps[h][:, :HEAD], so_far[h]) + jnp.where(
                    is_state, maps[h], 0.0
                )
    for h in every:
        whole_ref[h] = so_far[h].astype(narrow)


def in_vmem(count):
    return [pl.BlockSpec(memory_space=pltpu.VMEM)] * count


def scanned(*arrays):
    length, width = arrays[0].shape
    heads = width // HEAD
    return pl.pallas_call(
        scan_kernel,
        out_shape=(
            jax.ShapeDtypeStruct((heads, length, 2 * HEAD), jnp.float32),
            jax.ShapeDtypeStruct((heads, HEAD, 2 * HEAD), jnp.bfloat16),
        ),
        in_specs=in_vmem(6),
        out_specs=tuple(in_vmem(2)),
        cost_estimate=pl.CostEstimate(flops=4_000_000_000, bytes_accessed=1 << 20, transcendentals=0),
        name="scan_blocks",
    )(*arrays)


def finish_kernel(core_ref, out_ref, first_ref, reach_ref, gate_ref, gain_ref, gated_ref):
    wide = jnp.float32
    heads = out_ref.shape[0]
    later_core = core_ref[0] > 0
    parts = []
    for h in range(heads):
        before = first_ref[h].astype(wide)
        reach = reach_ref[h]
        passed = split_dot(before[:, :HEAD], reach) + before[:, HEAD:]
        reach = jnp.where(later_core, passed, reach)
        here = out_ref[h]
        mixed = split_dot(here[:, :HEAD], reach) + here[:, HEAD:]
        centre = mixed - jnp.mean(mixed, axis=1, keepdims=True)
        spread = jnp.mean(centre * centre, axis=1, keepdims=True)
        parts.append(centre * lax.rsqrt(spread + 0.00064))
    normed = jnp.concatenate(parts, axis=1) * gain_ref[...]
    gated_ref[...] = (normed * jax.nn.sigmoid(gate_ref[...].astype(wide))).astype(gated_ref.dtype)


def finished(outputs, first, reach, gate_logits, gain):
    core = lax.axis_index("sp_1").astype(jnp.int32).reshape(1)
    return pl.pallas_call(
        finish_kernel,
        out_shape=jax.ShapeDtypeStruct(gate_logits.shape, jnp.bfloat16),
        in_specs=[pl.BlockSpec(memory_space=pltpu.SMEM), *in_vmem(5)],
        out_specs=in_vmem(1)[0],
        cost_estimate=pl.CostEstimate(flops=400_000_000, bytes_accessed=1 << 19, transcendentals=0),
        name="finish_heads",
    )(core, outputs, first, reach, gate_logits, gain.reshape(1, -1))


def hidden_rows(rows, gate, up):
    gated = plain_dot(rows, gate)
    return (gated * jax.nn.sigmoid(gated) * plain_dot(rows, up)).astype(jnp.bfloat16)


def first_kernel(rows, gate, up, down, out, gates, ups, downs, hidden, sems):
    width, width_ff = gate.shape
    cuts = [pl.ds(f, min(FF_TILE, width_ff - f)) for f in range(0, width_ff, FF_TILE)]
    wide_cuts = [pl.ds(f, 2 * FF_TILE) for f in range(0, width, 2 * FF_TILE)]
    copies = []
    for which, (source, here) in enumerate(((gate, gates), (up, ups), (down, downs))):
        places = wide_cuts if which == 2 else cuts
        copies.append(
            [
                pltpu.make_async_copy(source.at[:, p], here.at[:, p], sems.at[which, n])
                for n, p in enumerate(places)
            ]
        )
    for n in range(len(cuts)):
        copies[0][n].start()
        copies[1][n].start()
    for one in copies[2]:
        one.start()
    for n, p in enumerate(cuts):
        copies[0][n].wait()
        copies[1][n].wait()
        hidden[:, p] = hidden_rows(rows[...], gates[:, p], ups[:, p])
    for n, p in enumerate(wide_cuts):
        copies[2][n].wait()
        out[:, p] = plain_dot(hidden[...], downs[:, p]).astype(out.dtype)


def first_rows(rows, gate, up, down):
    count, width = rows.shape
    width_ff = gate.shape[1]
    shapes = [jax.ShapeDtypeStruct(a.shape, a.dtype) for a in (rows, gate, up, down)]
    return pl.pallas_call(
        first_kernel,
        out_shape=tuple(shapes),
        in_specs=[in_vmem(1)[0], *[pl.BlockSpec(memory_space=pltpu.HBM)] * 3],
        out_specs=tuple(in_vmem(4)),
        scratch_shapes=[
            pltpu.VMEM((count, width_ff), jnp.bfloat16),
            pltpu.SemaphoreType.DMA((3, 4)),
        ],
        compiler_params=pltpu.CompilerParams(vmem_limit_bytes=LIMIT_FIRST << 20),
        cost_estimate=pl.CostEstimate(
            flops=6 * count * width * width_ff, bytes_accessed=6 * width * width_ff, transcendentals=0
        ),
        name="first_rows",
    )(rows, gate, up, down)


def more_kernel(count, *refs):
    pieces, (gates, ups, downs), (out, hidden) = refs[:count], refs[count : count + 3], refs[count + 3 :]
    width, width_ff = gates.shape
    rows = pieces[0][...]
    if count > 1:
        rows = jnp.concatenate([piece[...] for piece in pieces], axis=0)
    for f in range(0, width_ff, FF_TILE):
        p = slice(f, min(f + FF_TILE, width_ff))
        hidden[:, p] = hidden_rows(rows, gates[:, p], ups[:, p])
    for f in range(0, width, 2 * FF_TILE):
        p = slice(f, f + 2 * FF_TILE)
        out[:, p] = plain_dot(hidden[...], downs[:, p]).astype(out.dtype)


def more_rows(pieces, weights):
    count, width = sum(piece.shape[0] for piece in pieces), pieces[0].shape[1]
    width_ff = weights[0].shape[1]
    return pl.pallas_call(
        partial(more_kernel, len(pieces)),
        out_shape=jax.ShapeDtypeStruct((count, width), jnp.bfloat16),
        in_specs=in_vmem(len(pieces) + 3),
        out_specs=in_vmem(1)[0],
        scratch_shapes=[pltpu.VMEM((count, width_ff), jnp.bfloat16)],
        compiler_params=pltpu.CompilerParams(vmem_limit_bytes=LIMIT_REST << 20),
        cost_estimate=pl.CostEstimate(
            flops=6 * count * width * width_ff, bytes_accessed=6 * width * width_ff, transcendentals=0
        ),
        name="more_rows",
    )(*pieces, *weights)


def body(
    receptance,
    head_keys,
    head_values,
    decay_logits,
    decay_boost,
    correction_logits,
    gate_logits,
    head_norm_gain,
    output_weight,
    residual,
    expert_norm_gain,
    routes,
    routing_weight,
    expert_gate_weight,
    expert_up_weight,
    expert_down_weight,
):
    outputs, whole = scanned(
        receptance, head_keys, head_values, decay_logits, decay_boost, correction_logits
    )
    weights, whole = gathered_weight(output_weight, whole)
    first, reach = incoming_state(whole)
    gated = finished(outputs, first, reach, gate_logits, head_norm_gain)
    rows_here = own_rows(gated)
    branch = projected(rows_here, weights)
    stream = residual.astype(jnp.float32) + branch
    normal = (
        stream
        * lax.rsqrt(jnp.mean(stream * stream, axis=-1, keepdims=True) + 1e-06)
        * expert_norm_gain
    ).astype(jnp.bfloat16)
    sp_count = lax.axis_size(SP)
    tp_count = lax.axis_size("tp")
    capacity = max(2, 2 * TOK_DEV * TOP // (tp_count * sp_count))
    local_count = normal.shape[0]
    width_model = normal.shape[1]
    flat_routes = routes.reshape(-1)
    expert_ids = jnp.arange(sp_count, dtype=jnp.int32)
    chosen = (flat_routes[:, None] == expert_ids[None, :]).astype(jnp.int32)
    earlier = jnp.cumsum(chosen, axis=0) - chosen
    rank = jnp.sum(earlier * chosen, axis=1)
    place = flat_routes * capacity + rank
    places = jnp.arange(sp_count * capacity, dtype=jnp.int32)
    onehot = (place[:, None] == places[None, :]).astype(jnp.bfloat16)
    placed = jnp.sum(onehot.reshape(local_count, TOP, sp_count * capacity), axis=1)
    placed, onehot, routing_weight = lax.optimization_barrier((placed, onehot, routing_weight))
    outbound = jnp.einsum("ts,td->sd", placed, normal, preferred_element_type=jnp.float32).astype(
        jnp.bfloat16
    )
    going = outbound.reshape(sp_count, 2 * capacity, width_model // 2)
    arrived = lax.all_to_all(going, SP, split_axis=0, concat_axis=0, tiled=True)
    arrived = arrived.reshape(-1, width_model)
    back, ahead = shifted(arrived, "tp", 1), shifted(arrived, "tp", -1)
    weights = (expert_gate_weight[0], expert_up_weight[0], expert_down_weight[0])
    own, *weights = first_rows(arrived, *weights)
    middle = arrived.shape[0] // 2
    away = [shifted(back[:middle], "tp", 1), shifted(ahead[middle:], "tp", -1)]
    back = more_rows([back], weights)
    ahead = more_rows([ahead], weights)
    away = more_rows(away, weights)
    parts = [own]
    for piece, k in ((back, -1), (ahead, 1), (away, 2)):
        parts.append(shifted(piece, "tp", k))
    total = sum(piece.astype(jnp.float32) for piece in parts).astype(jnp.bfloat16)
    total = total.reshape(sp_count, 2 * capacity, width_model // 2)
    home = lax.all_to_all(total, SP, split_axis=0, concat_axis=0, tiled=True)
    home = home.reshape(-1, width_model)
    picked = jnp.dot(onehot, home, preferred_element_type=jnp.float32)
    routed = jnp.sum(
        picked.reshape(local_count, TOP, width_model) * routing_weight[:, :, None], axis=1
    )
    return (stream + routed).astype(jnp.bfloat16)


def solution(mesh):
    torus = Mesh(
        mesh.devices.reshape(mesh.shape["grp"], 16, 2, mesh.shape["tp"]),
        ("grp", "sp_0", "sp_1", "tp"),
    )
    return jax.shard_map(
        body,
        mesh=torus,
        in_specs=(
            P(GRP_SP, "tp"),
            P(GRP_SP, "tp"),
            P(GRP_SP, "tp"),
            P(GRP_SP, "tp"),
            P(GRP_SP, "tp"),
            P(GRP_SP, "tp"),
            P(GRP_SP, "tp"),
            P("tp"),
            P("tp", None),
            P(GRP_SP_TP, None),
            P(),
            P(GRP_SP_TP, None),
            P(GRP_SP_TP, None),
            P(SP, None, "tp"),
            P(SP, None, "tp"),
            P(SP, "tp", None),
        ),
        out_specs=P(GRP_SP_TP, None),
        check_vma=False,
    )
```

```python
import math
from functools import partial

import jax
import jax.numpy as jnp
from jax import lax
from jax.experimental import pallas as pl
from jax.experimental.pallas import tpu as pltpu
from jax.sharding import Mesh
from jax.sharding import PartitionSpec as P


HEAD = 64
TOP = 2
BLK = 32
QUAD = 4
OFFSETS = (1, 3, 2)
FF_TILE = 256
LIMIT_FIRST = 42
LIMIT_REST = 18
HALF_DOWN = math.exp(-0.5)
TOK_DEV = 128
SP = ("sp_0", "sp_1")
GRP_SP = ("grp", "sp_0", "sp_1")
GRP_SP_TP = ("grp", "sp_0", "sp_1", "tp")


highest = lax.Precision.HIGHEST


def shifted(x, axis, step):
    size = lax.axis_size(axis)
    return lax.ppermute(x, axis, [(i, (i + step) % size) for i in range(size)])


def within_quads(x, axis, step):
    size = lax.axis_size(axis)
    pairs = [(i, i // QUAD * QUAD + (i % QUAD + step) % QUAD) for i in range(size)]
    return lax.ppermute(x, axis, pairs)


def across_quads(x, axis, step):
    size = lax.axis_size(axis)
    return lax.ppermute(x, axis, [(i, i + step * QUAD) for i in range(size - step * QUAD)])


def after(later, earlier):
    moved = jnp.einsum("hij,hjk->hik", later[..., :HEAD], earlier, precision=highest)
    return moved + jnp.where(jnp.arange(2 * HEAD) < HEAD, 0.0, later)


def onto(later, state):
    moved = jnp.einsum("hij,hjk->hik", later[..., :HEAD], state, precision=highest)
    return moved + later[..., HEAD:]


def chip_kernel(core_ref, own_ref, other_ref, chip_ref, sent_ref):
    core = core_ref[0]
    half = chip_ref.shape[0]
    for h in range(half):
        own = own_ref[core * half + h].astype(jnp.float32)
        other = other_ref[core * half + h].astype(jnp.float32)
        first = jnp.where(core == 0, own, other)
        second = jnp.where(core == 0, other, own)
        state = lax.broadcasted_iota(jnp.int32, second.shape, 1) >= HEAD
        chip = split_dot(second[:, :HEAD], first) + jnp.where(state, second, 0.0)
        chip_ref[h] = chip
        sent_ref[h] = chip.astype(sent_ref.dtype)


def core_index():
    return lax.axis_index("sp_1").astype(jnp.int32).reshape(1)


def chip_map(own, other):
    shape = (own.shape[0] // 2, *own.shape[1:])
    return pl.pallas_call(
        chip_kernel,
        out_shape=(
            jax.ShapeDtypeStruct(shape, jnp.float32),
            jax.ShapeDtypeStruct(shape, jnp.bfloat16),
        ),
        in_specs=[pl.BlockSpec(memory_space=pltpu.SMEM), *in_vmem(2)],
        out_specs=tuple(in_vmem(2)),
        cost_estimate=pl.CostEstimate(flops=200_000_000, bytes_accessed=1 << 18, transcendentals=0),
        compiler_params=pltpu.CompilerParams(vmem_limit_bytes=8 << 20),
        name="chip_map",
    )(core_index(), own, other)


def incoming_state(packed):
    wide = jnp.float32
    other = shifted(packed, "sp_1", 1)
    chip, sent = chip_map(packed, other)
    member = lax.axis_index("sp_0") % QUAD
    came = [chip] + [within_quads(sent, "sp_0", k).astype(wide) for k in range(1, QUAD)]
    came = jnp.stack(came)
    total = lax.dynamic_index_in_dim(came, member % QUAD, 0, False)
    eye = jnp.eye(HEAD, 2 * HEAD, dtype=wide)
    before = jnp.where(member == 0, eye, total)
    for k in range(1, QUAD):
        piece = lax.dynamic_index_in_dim(came, (member - k) % QUAD, 0, False)
        total = after(piece, total)
        if k < QUAD - 1:
            before = jnp.where(member == k + 1, total, before)
    sent = total.astype(jnp.bfloat16)
    far = [across_quads(sent, "sp_0", k).astype(wide) for k in range(QUAD - 1, 0, -1)]
    reach = far[0][..., HEAD:]
    for piece in far[1:]:
        reach = onto(piece, reach)
    reach = onto(before, reach)
    mine = jnp.concatenate([reach[0], reach[1]], axis=1).astype(jnp.bfloat16)
    swapped = shifted(mine, "sp_1", 1)
    return other, mine, swapped


def gathered_weight(weight):
    half = weight.shape[1] // 2
    core = lax.axis_index("sp_1")
    mine = lax.dynamic_slice_in_dim(weight, core * half, half, 1)
    mine = [shifted(mine, "tp", k) for k in OFFSETS]
    other = [shifted(piece, "sp_1", 1) for piece in mine]
    return mine, other


def split_dot(first, second):
    high_a, high_b = first.astype(jnp.bfloat16), second.astype(jnp.bfloat16)
    low_a = (first - high_a.astype(jnp.float32)).astype(jnp.bfloat16)
    low_b = (second - high_b.astype(jnp.float32)).astype(jnp.bfloat16)
    return plain_dot(high_a, high_b) + (plain_dot(high_a, low_b) + plain_dot(low_a, high_b))


def plain_dot(first, second, dims=((1,), (0,))):
    return lax.dot_general(
        first.astype(jnp.bfloat16),
        second.astype(jnp.bfloat16),
        (dims, ((), ())),
        preferred_element_type=jnp.float32,
    )


def scan_kernel(query_ref, key_ref, value_ref, decay_ref, boost_ref, rate_ref, out_ref, whole_ref):
    wide, narrow = jnp.float32, jnp.bfloat16
    length, width = key_ref.shape
    heads = width // HEAD
    blocks = length // BLK
    keyed = key_ref[...].astype(wide)
    query = query_ref[...].astype(wide)
    valued = value_ref[...]
    lane_r = lax.broadcasted_iota(jnp.int32, (width, width), 0) // HEAD
    lane_c = lax.broadcasted_iota(jnp.int32, (width, width), 1) // HEAD
    same_head = (lane_r == lane_c).astype(narrow)
    square = keyed * keyed
    square_high = square.astype(narrow)
    square_low = (square - square_high.astype(wide)).astype(narrow)
    norm = plain_dot(square_high, same_head) + plain_dot(square_low, same_head)
    unit = keyed * lax.rsqrt(norm + 1e-06)
    insert = unit * jax.nn.sigmoid(rate_ref[...].astype(wide))
    slow = jax.nn.sigmoid(decay_ref[...].astype(wide)) * HALF_DOWN
    log_decay = boost_ref[...] - slow
    row = lax.broadcasted_iota(jnp.int32, (length, length), 0)
    col = lax.broadcasted_iota(jnp.int32, (length, length), 1)
    same_block = row // BLK == col // BLK
    strict = same_block & (row > col)
    inclusive = same_block & (row >= col)
    sums = jnp.concatenate([inclusive.astype(narrow), same_block.astype(narrow)], axis=0)
    part, added = log_decay, 0.0
    for _ in range(3):
        piece = part.astype(narrow)
        added = added + plain_dot(sums, piece)
        part = part - piece.astype(wide)
    upto, final = added[:length], added[length:]
    remove_scaled = -unit * jnp.exp(upto - log_decay)
    query_scaled = query * jnp.exp(upto)
    shrink = jnp.exp(-upto)
    insert_scaled = (insert * shrink).astype(narrow)
    key_scaled = (keyed * shrink).astype(narrow)
    tail = jnp.exp(final - upto)
    insert_tail = (insert * tail).astype(narrow)
    key_tail = (keyed * tail).astype(narrow)
    kept = jnp.exp(final)
    every = range(heads)
    lanes = [slice(h * HEAD, (h + 1) * HEAD) for h in every]
    pair = [
        plain_dot(
            jnp.concatenate([remove_scaled[:, lanes[h]], query_scaled[:, lanes[h]]], axis=0),
            jnp.concatenate([insert_scaled[:, lanes[h]], key_scaled[:, lanes[h]]], axis=0),
            ((1,), (1,)),
        )
        for h in every
    ]
    among = [jnp.where(strict, pair[h][:length, :length], 0.0).astype(narrow) for h in every]
    read = [jnp.where(inclusive, pair[h][length:, :length], 0.0).astype(narrow) for h in every]
    by_keys = [
        jnp.concatenate(
            [
                jnp.where(strict, pair[h][:length, length:], 0.0),
                jnp.where(inclusive, pair[h][length:, length:], 0.0),
            ],
            axis=0,
        ).astype(narrow)
        for h in every
    ]
    from_values = [plain_dot(by_keys[h], valued[:, lanes[h]]) for h in every]
    solved = [
        jnp.concatenate([remove_scaled[:, lanes[h]], from_values[h][:length]], axis=1)
        for h in every
    ]
    power = among
    covered = 1
    while covered < BLK:
        solved = [solved[h] + plain_dot(power[h], solved[h]) for h in every]
        covered = 2 * covered
        if covered < BLK:
            power = [plain_dot(power[h], power[h]).astype(narrow) for h in every]
    reading = [
        jnp.concatenate([query_scaled[:, lanes[h]], from_values[h][length:]], axis=1)
        + plain_dot(read[h], solved[h])
        for h in every
    ]
    wide_r = lax.broadcasted_iota(jnp.int32, (HEAD, 2 * HEAD), 0)
    wide_c = lax.broadcasted_iota(jnp.int32, (HEAD, 2 * HEAD), 1)
    diagonal = wide_r == wide_c
    is_state = wide_c >= HEAD
    none = jnp.zeros((BLK, HEAD), narrow)
    so_far = [None] * heads
    for n in range(blocks):
        rows = slice(n * BLK, (n + 1) * BLK)
        maps = []
        for h in every:
            sources = jnp.concatenate([insert_tail[rows, lanes[h]], key_tail[rows, lanes[h]]], axis=0)
            targets = jnp.concatenate(
                [
                    solved[h][rows].astype(narrow),
                    jnp.concatenate([none, valued[rows, lanes[h]]], axis=1),
                ],
                axis=0,
            )
            keeps = kept[n * BLK : n * BLK + 1, lanes[h]]
            keeps = jnp.concatenate([keeps, keeps], axis=1)
            maps.append(
                plain_dot(sources, targets, ((0,), (0,))) + jnp.where(diagonal, keeps, 0.0)
            )
        for h in every:
            here = reading[h][rows]
            if n == 0:
                out_ref[h, rows, :] = here
                so_far[h] = maps[h]
            else:
                moved = split_dot(here[:, :HEAD], so_far[h])
                local = lax.broadcasted_iota(jnp.int32, here.shape, 1) >= HEAD
                out_ref[h, rows, :] = moved + jnp.where(local, here, 0.0)
                so_far[h] = split_dot(maps[h][:, :HEAD], so_far[h]) + jnp.where(
                    is_state, maps[h], 0.0
                )
    for h in every:
        whole_ref[h] = so_far[h].astype(narrow)


def in_vmem(count):
    return [pl.BlockSpec(memory_space=pltpu.VMEM)] * count


def scanned(*arrays):
    length, width = arrays[0].shape
    heads = width // HEAD
    return pl.pallas_call(
        scan_kernel,
        out_shape=(
            jax.ShapeDtypeStruct((heads, length, 2 * HEAD), jnp.float32),
            jax.ShapeDtypeStruct((heads, HEAD, 2 * HEAD), jnp.bfloat16),
        ),
        in_specs=in_vmem(6),
        out_specs=tuple(in_vmem(2)),
        cost_estimate=pl.CostEstimate(flops=4_000_000_000, bytes_accessed=1 << 20, transcendentals=0),
        name="scan_blocks",
    )(*arrays)


def finish_kernel(
    place_ref, out_ref, first_ref, mine_ref, swapped_ref, gate_ref, gain_ref, *refs
):
    *blocks, gated_ref = refs
    wide = jnp.float32
    heads = out_ref.shape[0]
    later_core = place_ref[0] > 0
    mine, swapped = mine_ref[...].astype(wide), swapped_ref[...].astype(wide)
    low = jnp.where(later_core, swapped, mine)
    high = jnp.where(later_core, mine, swapped)
    parts = []
    for h in range(heads):
        before = first_ref[h].astype(wide)
        reach = (low, high)[h // 2][:, h % 2 * HEAD : (h % 2 + 1) * HEAD]
        passed = split_dot(before[:, :HEAD], reach) + before[:, HEAD:]
        reach = jnp.where(later_core, passed, reach)
        here = out_ref[h]
        mixed = split_dot(here[:, :HEAD], reach) + here[:, HEAD:]
        centre = mixed - jnp.mean(mixed, axis=1, keepdims=True)
        spread = jnp.mean(centre * centre, axis=1, keepdims=True)
        parts.append(centre * lax.rsqrt(spread + 0.00064))
    normed = jnp.concatenate(parts, axis=1) * gain_ref[...]
    gated_ref[...] = normed * jax.nn.sigmoid(gate_ref[...].astype(wide))
    count = blocks[0].shape[0]
    for block, k in zip(blocks, (0, *OFFSETS)):
        start = (place_ref[1] + k) % len(blocks) * count
        block[...] = gated_ref[pl.ds(pl.multiple_of(start, count), count), :].astype(block.dtype)


def finished(outputs, first, mine, swapped, gate_logits, gain):
    count = lax.axis_size("tp")
    rows, width = gate_logits.shape
    place = jnp.stack([lax.axis_index("sp_1"), lax.axis_index("tp")]).astype(jnp.int32)
    block = jax.ShapeDtypeStruct((rows // count, width), jnp.bfloat16)
    return pl.pallas_call(
        finish_kernel,
        out_shape=(block,) * count,
        in_specs=[pl.BlockSpec(memory_space=pltpu.SMEM), *in_vmem(6)],
        out_specs=tuple(in_vmem(count)),
        scratch_shapes=[pltpu.VMEM((rows, width), jnp.float32)],
        cost_estimate=pl.CostEstimate(flops=400_000_000, bytes_accessed=1 << 19, transcendentals=0),
        compiler_params=pltpu.CompilerParams(vmem_limit_bytes=12 << 20),
        name="finish_heads",
    )(place, outputs, first, mine, swapped, gate_logits, gain.reshape(1, -1))


def project_kernel(count, core_ref, own_ref, weight_ref, *refs):
    rows, mine, other = refs[:count], refs[count : 2 * count], refs[2 * count : 3 * count]
    residual_ref, gain_ref, placed_ref, stream_ref, out_ref = refs[3 * count :]
    halves = []
    for side in (mine, other):
        halves.append(sum(plain_dot(r[...], w[...]) for r, w in zip(rows, side)))
    swap = core_ref[0] > 0
    left = jnp.where(swap, halves[1], halves[0])
    right = jnp.where(swap, halves[0], halves[1])
    branch = plain_dot(own_ref[...], weight_ref[...]) + jnp.concatenate([left, right], axis=1)
    stream = residual_ref[...].astype(jnp.float32) + branch
    stream_ref[...] = stream
    scale = lax.rsqrt(jnp.mean(stream * stream, axis=1, keepdims=True) + 1e-06)
    normal = (stream * scale * gain_ref[...]).astype(jnp.bfloat16)
    out_ref[...] = plain_dot(placed_ref[...], normal, ((0,), (0,))).astype(out_ref.dtype)


def projected(own, weight, rows, weights, residual, gain, placed):
    count, width = len(rows), residual.shape[1]
    return pl.pallas_call(
        partial(project_kernel, count),
        out_shape=(
            jax.ShapeDtypeStruct(residual.shape, jnp.float32),
            jax.ShapeDtypeStruct((placed.shape[1], width), jnp.bfloat16),
        ),
        in_specs=[pl.BlockSpec(memory_space=pltpu.SMEM), *in_vmem(3 * count + 5)],
        out_specs=tuple(in_vmem(2)),
        cost_estimate=pl.CostEstimate(flops=800_000_000, bytes_accessed=5 << 20, transcendentals=0),
        compiler_params=pltpu.CompilerParams(vmem_limit_bytes=20 << 20),
        name="project_rows",
    )(core_index(), own, weight, *rows, *weights[0], *weights[1], residual, gain.reshape(1, -1), placed)


def hidden_rows(rows, gate, up):
    gated = plain_dot(rows, gate)
    return (gated * jax.nn.sigmoid(gated) * plain_dot(rows, up)).astype(jnp.bfloat16)


def first_kernel(rows, gate, up, down, out, gates, ups, downs, hidden, sems):
    width, width_ff = gate.shape
    cuts = [pl.ds(f, min(FF_TILE, width_ff - f)) for f in range(0, width_ff, FF_TILE)]
    wide_cuts = [pl.ds(f, 2 * FF_TILE) for f in range(0, width, 2 * FF_TILE)]
    copies = []
    for which, (source, here) in enumerate(((gate, gates), (up, ups), (down, downs))):
        places = wide_cuts if which == 2 else cuts
        copies.append(
            [
                pltpu.make_async_copy(source.at[:, p], here.at[:, p], sems.at[which, n])
                for n, p in enumerate(places)
            ]
        )
    for n in range(len(cuts)):
        copies[0][n].start()
        copies[1][n].start()
    for one in copies[2]:
        one.start()
    for n, p in enumerate(cuts):
        copies[0][n].wait()
        copies[1][n].wait()
        hidden[:, p] = hidden_rows(rows[...], gates[:, p], ups[:, p])
    for n, p in enumerate(wide_cuts):
        copies[2][n].wait()
        out[:, p] = plain_dot(hidden[...], downs[:, p]).astype(out.dtype)


def first_rows(rows, gate, up, down):
    count, width = rows.shape
    width_ff = gate.shape[1]
    shapes = [jax.ShapeDtypeStruct(a.shape, a.dtype) for a in (rows, gate, up, down)]
    return pl.pallas_call(
        first_kernel,
        out_shape=tuple(shapes),
        in_specs=[in_vmem(1)[0], *[pl.BlockSpec(memory_space=pltpu.HBM)] * 3],
        out_specs=tuple(in_vmem(4)),
        scratch_shapes=[
            pltpu.VMEM((count, width_ff), jnp.bfloat16),
            pltpu.SemaphoreType.DMA((3, 4)),
        ],
        compiler_params=pltpu.CompilerParams(vmem_limit_bytes=LIMIT_FIRST << 20),
        cost_estimate=pl.CostEstimate(
            flops=6 * count * width * width_ff, bytes_accessed=6 * width * width_ff, transcendentals=0
        ),
        name="first_rows",
    )(rows, gate, up, down)


def more_kernel(count, *refs):
    pieces, (gates, ups, downs), (out, hidden) = refs[:count], refs[count : count + 3], refs[count + 3 :]
    width, width_ff = gates.shape
    rows = pieces[0][...]
    if count > 1:
        rows = jnp.concatenate([piece[...] for piece in pieces], axis=0)
    for f in range(0, width_ff, FF_TILE):
        p = slice(f, min(f + FF_TILE, width_ff))
        hidden[:, p] = hidden_rows(rows, gates[:, p], ups[:, p])
    for f in range(0, width, 2 * FF_TILE):
        p = slice(f, f + 2 * FF_TILE)
        out[:, p] = plain_dot(hidden[...], downs[:, p]).astype(out.dtype)


def more_rows(pieces, weights):
    count, width = sum(piece.shape[0] for piece in pieces), pieces[0].shape[1]
    width_ff = weights[0].shape[1]
    return pl.pallas_call(
        partial(more_kernel, len(pieces)),
        out_shape=jax.ShapeDtypeStruct((count, width), jnp.bfloat16),
        in_specs=in_vmem(len(pieces) + 3),
        out_specs=in_vmem(1)[0],
        scratch_shapes=[pltpu.VMEM((count, width_ff), jnp.bfloat16)],
        compiler_params=pltpu.CompilerParams(vmem_limit_bytes=LIMIT_REST << 20),
        cost_estimate=pl.CostEstimate(
            flops=6 * count * width * width_ff, bytes_accessed=6 * width * width_ff, transcendentals=0
        ),
        name="more_rows",
    )(*pieces, *weights)


def body(
    receptance,
    head_keys,
    head_values,
    decay_logits,
    decay_boost,
    correction_logits,
    gate_logits,
    head_norm_gain,
    output_weight,
    residual,
    expert_norm_gain,
    routes,
    routing_weight,
    expert_gate_weight,
    expert_up_weight,
    expert_down_weight,
):
    outputs, whole = scanned(
        receptance, head_keys, head_values, decay_logits, decay_boost, correction_logits
    )
    weights = gathered_weight(output_weight)
    first, mine, swapped = incoming_state(whole)
    own, *blocks = finished(outputs, first, mine, swapped, gate_logits, head_norm_gain)
    rows_here = [shifted(b, "tp", k) for b, k in zip(blocks, OFFSETS)]
    sp_count = lax.axis_size(SP)
    tp_count = lax.axis_size("tp")
    capacity = max(2, 2 * TOK_DEV * TOP // (tp_count * sp_count))
    local_count, width_model = residual.shape
    flat_routes = routes.reshape(-1)
    expert_ids = jnp.arange(sp_count, dtype=jnp.int32)
    chosen = (flat_routes[:, None] == expert_ids[None, :]).astype(jnp.int32)
    earlier = jnp.cumsum(chosen, axis=0) - chosen
    rank = jnp.sum(earlier * chosen, axis=1)
    place = flat_routes * capacity + rank
    places = jnp.arange(sp_count * capacity, dtype=jnp.int32)
    onehot = (place[:, None] == places[None, :]).astype(jnp.bfloat16)
    placed = jnp.sum(onehot.reshape(local_count, TOP, sp_count * capacity), axis=1)
    placed, onehot, routing_weight = lax.optimization_barrier((placed, onehot, routing_weight))
    stream, outbound = projected(
        own, output_weight, rows_here, weights, residual, expert_norm_gain, placed
    )
    going = outbound.reshape(sp_count, 2 * capacity, width_model // 2)
    arrived = lax.all_to_all(going, SP, split_axis=0, concat_axis=0, tiled=True)
    arrived = arrived.reshape(-1, width_model)
    back, ahead = shifted(arrived, "tp", 1), shifted(arrived, "tp", -1)
    weights = (expert_gate_weight[0], expert_up_weight[0], expert_down_weight[0])
    own, *weights = first_rows(arrived, *weights)
    middle = arrived.shape[0] // 2
    away = [shifted(back[:middle], "tp", 1), shifted(ahead[middle:], "tp", -1)]
    back = more_rows([back], weights)
    ahead = more_rows([ahead], weights)
    away = more_rows(away, weights)
    parts = [own]
    for piece, k in ((back, -1), (ahead, 1), (away, 2)):
        parts.append(shifted(piece, "tp", k))
    total = sum(piece.astype(jnp.float32) for piece in parts).astype(jnp.bfloat16)
    total = total.reshape(sp_count, 2 * capacity, width_model // 2)
    home = lax.all_to_all(total, SP, split_axis=0, concat_axis=0, tiled=True)
    home = home.reshape(-1, width_model)
    picked = jnp.dot(onehot, home, preferred_element_type=jnp.float32)
    routed = jnp.sum(
        picked.reshape(local_count, TOP, width_model) * routing_weight[:, :, None], axis=1
    )
    return (stream + routed).astype(jnp.bfloat16)


def solution(mesh):
    torus = Mesh(
        mesh.devices.reshape(mesh.shape["grp"], 16, 2, mesh.shape["tp"]),
        ("grp", "sp_0", "sp_1", "tp"),
    )
    return jax.shard_map(
        body,
        mesh=torus,
        in_specs=(
            P(GRP_SP, "tp"),
            P(GRP_SP, "tp"),
            P(GRP_SP, "tp"),
            P(GRP_SP, "tp"),
            P(GRP_SP, "tp"),
            P(GRP_SP, "tp"),
            P(GRP_SP, "tp"),
            P("tp"),
            P("tp", None),
            P(GRP_SP_TP, None),
            P(),
            P(GRP_SP_TP, None),
            P(GRP_SP_TP, None),
            P(SP, None, "tp"),
            P(SP, None, "tp"),
            P(SP, "tp", None),
        ),
        out_specs=P(GRP_SP_TP, None),
        check_vma=False,
    )
```

```python
import math
from functools import partial

import jax
import jax.numpy as jnp
from jax import lax
from jax.experimental import pallas as pl
from jax.experimental.pallas import tpu as pltpu
from jax.sharding import Mesh
from jax.sharding import PartitionSpec as P


HEAD = 64
TOP = 2
BLK = 32
QUAD = 4
OFFSETS = (1, 3, 2)
FF_TILE = 256
LIMIT_FIRST = 42
LIMIT_REST = 18
HALF_DOWN = math.exp(-0.5)
TOK_DEV = 128
SP = ("sp_0", "sp_1")
GRP_SP = ("grp", "sp_0", "sp_1")
GRP_SP_TP = ("grp", "sp_0", "sp_1", "tp")


def shifted(x, axis, step):
    size = lax.axis_size(axis)
    return lax.ppermute(x, axis, [(i, (i + step) % size) for i in range(size)])


def within_quads(x, axis, step):
    size = lax.axis_size(axis)
    pairs = [(i, i // QUAD * QUAD + (i % QUAD + step) % QUAD) for i in range(size)]
    return lax.ppermute(x, axis, pairs)


def across_quads(x, axis, step):
    size = lax.axis_size(axis)
    return lax.ppermute(x, axis, [(i, i + step * QUAD) for i in range(size - step * QUAD)])


def chip_kernel(core_ref, own_ref, other_ref, chip_ref, sent_ref):
    core = core_ref[0]
    half = chip_ref.shape[0]
    for h in range(half):
        own = own_ref[core * half + h].astype(jnp.float32)
        other = other_ref[core * half + h].astype(jnp.float32)
        first = jnp.where(core == 0, own, other)
        second = jnp.where(core == 0, other, own)
        chip = joined(second, first)
        chip_ref[h] = chip
        sent_ref[h] = chip.astype(sent_ref.dtype)


def core_index():
    return lax.axis_index("sp_1").astype(jnp.int32).reshape(1)


def chip_map(own, other):
    shape = (own.shape[0] // 2, *own.shape[1:])
    return pl.pallas_call(
        chip_kernel,
        out_shape=(
            jax.ShapeDtypeStruct(shape, jnp.float32),
            jax.ShapeDtypeStruct(shape, jnp.bfloat16),
        ),
        in_specs=[pl.BlockSpec(memory_space=pltpu.SMEM), *in_vmem(2)],
        out_specs=tuple(in_vmem(2)),
        cost_estimate=pl.CostEstimate(flops=200_000_000, bytes_accessed=1 << 18, transcendentals=0),
        compiler_params=pltpu.CompilerParams(vmem_limit_bytes=8 << 20),
        name="chip_map",
    )(core_index(), own, other)


def joined(later, earlier):
    state = lax.broadcasted_iota(jnp.int32, later.shape, 1) >= HEAD
    return split_dot(later[:, :HEAD], earlier) + jnp.where(state, later, 0.0)


def quad_kernel(member_ref, chip_ref, *refs):
    *came, before_ref, sent_ref = refs
    member = member_ref[0]
    for h in range(chip_ref.shape[0]):
        pieces = [chip_ref[h]] + [piece[h].astype(jnp.float32) for piece in came]
        ordered = []
        for place in range(QUAD):
            piece = pieces[0]
            for k in range(1, QUAD):
                piece = jnp.where(member == (place + k) % QUAD, pieces[k], piece)
            ordered.append(piece)
        total = ordered[0]
        row = lax.broadcasted_iota(jnp.int32, total.shape, 0)
        col = lax.broadcasted_iota(jnp.int32, total.shape, 1)
        before = jnp.where(member == 0, (row == col).astype(jnp.float32), total)
        for place in range(1, QUAD):
            total = joined(ordered[place], total)
            if place < QUAD - 1:
                before = jnp.where(member == place + 1, total, before)
        before_ref[h] = before
        sent_ref[h] = total.astype(sent_ref.dtype)


def quad_map(chip, came):
    member = (lax.axis_index("sp_0") % QUAD).astype(jnp.int32).reshape(1)
    return pl.pallas_call(
        quad_kernel,
        out_shape=(
            jax.ShapeDtypeStruct(chip.shape, jnp.float32),
            jax.ShapeDtypeStruct(chip.shape, jnp.bfloat16),
        ),
        in_specs=[pl.BlockSpec(memory_space=pltpu.SMEM), *in_vmem(QUAD)],
        out_specs=tuple(in_vmem(2)),
        compiler_params=pltpu.CompilerParams(vmem_limit_bytes=8 << 20),
        cost_estimate=pl.CostEstimate(flops=200_000_000, bytes_accessed=1 << 18, transcendentals=0),
        name="quad_map",
    )(member, chip, *came)


def far_kernel(before_ref, *refs):
    *far, mine_ref = refs
    wide = jnp.float32
    for h in range(before_ref.shape[0]):
        reach = far[0][h][:, HEAD:].astype(wide)
        for piece in [*far[1:], before_ref]:
            later = piece[h].astype(wide)
            reach = split_dot(later[:, :HEAD], reach) + later[:, HEAD:]
        mine_ref[:, h * HEAD : (h + 1) * HEAD] = reach.astype(mine_ref.dtype)


def far_state(before, far):
    heads = before.shape[0]
    return pl.pallas_call(
        far_kernel,
        out_shape=jax.ShapeDtypeStruct((HEAD, heads * HEAD), jnp.bfloat16),
        in_specs=in_vmem(QUAD),
        out_specs=in_vmem(1)[0],
        compiler_params=pltpu.CompilerParams(vmem_limit_bytes=8 << 20),
        cost_estimate=pl.CostEstimate(flops=200_000_000, bytes_accessed=1 << 18, transcendentals=0),
        name="far_state",
    )(before, *far)


def incoming_state(packed):
    other = shifted(packed, "sp_1", 1)
    chip, sent = chip_map(packed, other)
    came = [within_quads(sent, "sp_0", k) for k in range(1, QUAD)]
    before, sent = quad_map(chip, came)
    far = [across_quads(sent, "sp_0", k) for k in range(QUAD - 1, 0, -1)]
    mine = far_state(before, far)
    swapped = shifted(mine, "sp_1", 1)
    return other, mine, swapped


def gathered_weight(weight):
    half = weight.shape[1] // 2
    core = lax.axis_index("sp_1")
    mine = lax.dynamic_slice_in_dim(weight, core * half, half, 1)
    mine = [shifted(mine, "tp", k) for k in OFFSETS]
    other = [shifted(piece, "sp_1", 1) for piece in mine]
    return mine, other


def split_dot(first, second):
    high_a, high_b = first.astype(jnp.bfloat16), second.astype(jnp.bfloat16)
    low_a = (first - high_a.astype(jnp.float32)).astype(jnp.bfloat16)
    low_b = (second - high_b.astype(jnp.float32)).astype(jnp.bfloat16)
    return plain_dot(high_a, high_b) + (plain_dot(high_a, low_b) + plain_dot(low_a, high_b))


def plain_dot(first, second, dims=((1,), (0,))):
    return lax.dot_general(
        first.astype(jnp.bfloat16),
        second.astype(jnp.bfloat16),
        (dims, ((), ())),
        preferred_element_type=jnp.float32,
    )


def scan_kernel(query_ref, key_ref, value_ref, decay_ref, boost_ref, rate_ref, out_ref, whole_ref):
    wide, narrow = jnp.float32, jnp.bfloat16
    length, width = key_ref.shape
    heads = width // HEAD
    blocks = length // BLK
    keyed = key_ref[...].astype(wide)
    query = query_ref[...].astype(wide)
    valued = value_ref[...]
    lane_r = lax.broadcasted_iota(jnp.int32, (width, width), 0) // HEAD
    lane_c = lax.broadcasted_iota(jnp.int32, (width, width), 1) // HEAD
    same_head = (lane_r == lane_c).astype(narrow)
    square = keyed * keyed
    square_high = square.astype(narrow)
    square_low = (square - square_high.astype(wide)).astype(narrow)
    norm = plain_dot(square_high, same_head) + plain_dot(square_low, same_head)
    unit = keyed * lax.rsqrt(norm + 1e-06)
    insert = unit * jax.nn.sigmoid(rate_ref[...].astype(wide))
    slow = jax.nn.sigmoid(decay_ref[...].astype(wide)) * HALF_DOWN
    log_decay = boost_ref[...] - slow
    row = lax.broadcasted_iota(jnp.int32, (length, length), 0)
    col = lax.broadcasted_iota(jnp.int32, (length, length), 1)
    same_block = row // BLK == col // BLK
    strict = same_block & (row > col)
    inclusive = same_block & (row >= col)
    sums = jnp.concatenate([inclusive.astype(narrow), same_block.astype(narrow)], axis=0)
    part, added = log_decay, 0.0
    for _ in range(3):
        piece = part.astype(narrow)
        added = added + plain_dot(sums, piece)
        part = part - piece.astype(wide)
    upto, final = added[:length], added[length:]
    remove_scaled = -unit * jnp.exp(upto - log_decay)
    query_scaled = query * jnp.exp(upto)
    shrink = jnp.exp(-upto)
    insert_scaled = (insert * shrink).astype(narrow)
    key_scaled = (keyed * shrink).astype(narrow)
    tail = jnp.exp(final - upto)
    insert_tail = (insert * tail).astype(narrow)
    key_tail = (keyed * tail).astype(narrow)
    kept = jnp.exp(final)
    every = range(heads)
    lanes = [slice(h * HEAD, (h + 1) * HEAD) for h in every]
    pair = [
        plain_dot(
            jnp.concatenate([remove_scaled[:, lanes[h]], query_scaled[:, lanes[h]]], axis=0),
            jnp.concatenate([insert_scaled[:, lanes[h]], key_scaled[:, lanes[h]]], axis=0),
            ((1,), (1,)),
        )
        for h in every
    ]
    among = [jnp.where(strict, pair[h][:length, :length], 0.0).astype(narrow) for h in every]
    read = [jnp.where(inclusive, pair[h][length:, :length], 0.0).astype(narrow) for h in every]
    by_keys = [
        jnp.concatenate(
            [
                jnp.where(strict, pair[h][:length, length:], 0.0),
                jnp.where(inclusive, pair[h][length:, length:], 0.0),
            ],
            axis=0,
        ).astype(narrow)
        for h in every
    ]
    from_values = [plain_dot(by_keys[h], valued[:, lanes[h]]) for h in every]
    solved = [
        jnp.concatenate([remove_scaled[:, lanes[h]], from_values[h][:length]], axis=1)
        for h in every
    ]
    power = among
    covered = 1
    while covered < BLK:
        solved = [solved[h] + plain_dot(power[h], solved[h]) for h in every]
        covered = 2 * covered
        if covered < BLK:
            power = [plain_dot(power[h], power[h]).astype(narrow) for h in every]
    reading = [
        jnp.concatenate([query_scaled[:, lanes[h]], from_values[h][length:]], axis=1)
        + plain_dot(read[h], solved[h])
        for h in every
    ]
    wide_r = lax.broadcasted_iota(jnp.int32, (HEAD, 2 * HEAD), 0)
    wide_c = lax.broadcasted_iota(jnp.int32, (HEAD, 2 * HEAD), 1)
    diagonal = wide_r == wide_c
    is_state = wide_c >= HEAD
    none = jnp.zeros((BLK, HEAD), narrow)
    so_far = [None] * heads
    for n in range(blocks):
        rows = slice(n * BLK, (n + 1) * BLK)
        maps = []
        for h in every:
            sources = jnp.concatenate([insert_tail[rows, lanes[h]], key_tail[rows, lanes[h]]], axis=0)
            targets = jnp.concatenate(
                [
                    solved[h][rows].astype(narrow),
                    jnp.concatenate([none, valued[rows, lanes[h]]], axis=1),
                ],
                axis=0,
            )
            keeps = kept[n * BLK : n * BLK + 1, lanes[h]]
            keeps = jnp.concatenate([keeps, keeps], axis=1)
            maps.append(
                plain_dot(sources, targets, ((0,), (0,))) + jnp.where(diagonal, keeps, 0.0)
            )
        for h in every:
            here = reading[h][rows]
            if n == 0:
                out_ref[h, rows, :] = here
                so_far[h] = maps[h]
            else:
                moved = split_dot(here[:, :HEAD], so_far[h])
                local = lax.broadcasted_iota(jnp.int32, here.shape, 1) >= HEAD
                out_ref[h, rows, :] = moved + jnp.where(local, here, 0.0)
                so_far[h] = split_dot(maps[h][:, :HEAD], so_far[h]) + jnp.where(
                    is_state, maps[h], 0.0
                )
    for h in every:
        whole_ref[h] = so_far[h].astype(narrow)


def in_vmem(count):
    return [pl.BlockSpec(memory_space=pltpu.VMEM)] * count


def scanned(*arrays):
    length, width = arrays[0].shape
    heads = width // HEAD
    return pl.pallas_call(
        scan_kernel,
        out_shape=(
            jax.ShapeDtypeStruct((heads, length, 2 * HEAD), jnp.float32),
            jax.ShapeDtypeStruct((heads, HEAD, 2 * HEAD), jnp.bfloat16),
        ),
        in_specs=in_vmem(6),
        out_specs=tuple(in_vmem(2)),
        cost_estimate=pl.CostEstimate(flops=4_000_000_000, bytes_accessed=1 << 20, transcendentals=0),
        name="scan_blocks",
    )(*arrays)


def finish_kernel(
    place_ref, out_ref, first_ref, mine_ref, swapped_ref, gate_ref, gain_ref, *refs
):
    *blocks, gated_ref = refs
    wide = jnp.float32
    heads = out_ref.shape[0]
    later_core = place_ref[0] > 0
    mine, swapped = mine_ref[...].astype(wide), swapped_ref[...].astype(wide)
    low = jnp.where(later_core, swapped, mine)
    high = jnp.where(later_core, mine, swapped)
    parts = []
    for h in range(heads):
        before = first_ref[h].astype(wide)
        reach = (low, high)[h // 2][:, h % 2 * HEAD : (h % 2 + 1) * HEAD]
        passed = split_dot(before[:, :HEAD], reach) + before[:, HEAD:]
        reach = jnp.where(later_core, passed, reach)
        here = out_ref[h]
        mixed = split_dot(here[:, :HEAD], reach) + here[:, HEAD:]
        centre = mixed - jnp.mean(mixed, axis=1, keepdims=True)
        spread = jnp.mean(centre * centre, axis=1, keepdims=True)
        parts.append(centre * lax.rsqrt(spread + 0.00064))
    normed = jnp.concatenate(parts, axis=1) * gain_ref[...]
    gated_ref[...] = normed * jax.nn.sigmoid(gate_ref[...].astype(wide))
    count = blocks[0].shape[0]
    for block, k in zip(blocks, (0, *OFFSETS)):
        start = (place_ref[1] + k) % len(blocks) * count
        block[...] = gated_ref[pl.ds(pl.multiple_of(start, count), count), :].astype(block.dtype)


def finished(outputs, first, mine, swapped, gate_logits, gain):
    count = lax.axis_size("tp")
    rows, width = gate_logits.shape
    place = jnp.stack([lax.axis_index("sp_1"), lax.axis_index("tp")]).astype(jnp.int32)
    block = jax.ShapeDtypeStruct((rows // count, width), jnp.bfloat16)
    return pl.pallas_call(
        finish_kernel,
        out_shape=(block,) * count,
        in_specs=[pl.BlockSpec(memory_space=pltpu.SMEM), *in_vmem(6)],
        out_specs=tuple(in_vmem(count)),
        scratch_shapes=[pltpu.VMEM((rows, width), jnp.float32)],
        cost_estimate=pl.CostEstimate(flops=400_000_000, bytes_accessed=1 << 19, transcendentals=0),
        compiler_params=pltpu.CompilerParams(vmem_limit_bytes=12 << 20),
        name="finish_heads",
    )(place, outputs, first, mine, swapped, gate_logits, gain.reshape(1, -1))


def project_kernel(count, capacity, core_ref, own_ref, weight_ref, *refs):
    rows, mine, other = refs[:count], refs[count : 2 * count], refs[2 * count : 3 * count]
    residual_ref, gain_ref, column_ref, line_ref, stream_ref, out_ref, onehot_ref = refs[3 * count :]
    halves = []
    for side in (mine, other):
        halves.append(sum(plain_dot(r[...], w[...]) for r, w in zip(rows, side)))
    swap = core_ref[0] > 0
    left = jnp.where(swap, halves[1], halves[0])
    right = jnp.where(swap, halves[0], halves[1])
    branch = plain_dot(own_ref[...], weight_ref[...]) + jnp.concatenate([left, right], axis=1)
    stream = residual_ref[...].astype(jnp.float32) + branch
    stream_ref[...] = stream
    scale = lax.rsqrt(jnp.mean(stream * stream, axis=1, keepdims=True) + 1e-06)
    normal = (stream * scale * gain_ref[...]).astype(jnp.bfloat16)
    tokens, total = stream.shape[0], line_ref.shape[1]
    expert = column_ref[...]
    row = lax.broadcasted_iota(jnp.int32, (total, total), 0)
    col = lax.broadcasted_iota(jnp.int32, (total, total), 1)
    earlier = (expert == line_ref[...]) & (col < row)
    rank = jnp.sum(earlier.astype(jnp.float32), axis=1, keepdims=True).astype(jnp.int32)
    slot = lax.broadcasted_iota(jnp.int32, onehot_ref.shape, 1)
    onehot = (expert * capacity + rank == slot).astype(jnp.float32)
    onehot_ref[...] = onehot.astype(onehot_ref.dtype)
    placed = sum(onehot[k : k + tokens] for k in range(0, total, tokens))
    out_ref[...] = plain_dot(placed, normal, ((0,), (0,))).astype(out_ref.dtype)


def projected(own, weight, rows, weights, residual, gain, routes, experts, capacity):
    count, width = len(rows), residual.shape[1]
    flat = routes.T.reshape(-1)
    return pl.pallas_call(
        partial(project_kernel, count, capacity),
        out_shape=(
            jax.ShapeDtypeStruct(residual.shape, jnp.float32),
            jax.ShapeDtypeStruct((experts * capacity, width), jnp.bfloat16),
            jax.ShapeDtypeStruct((routes.size, experts * capacity), jnp.bfloat16),
        ),
        in_specs=[pl.BlockSpec(memory_space=pltpu.SMEM), *in_vmem(3 * count + 6)],
        out_specs=tuple(in_vmem(3)),
        cost_estimate=pl.CostEstimate(flops=800_000_000, bytes_accessed=5 << 20, transcendentals=0),
        compiler_params=pltpu.CompilerParams(vmem_limit_bytes=20 << 20),
        name="project_rows",
    )(core_index(), own, weight, *rows, *weights[0], *weights[1], residual, gain.reshape(1, -1), flat.reshape(-1, 1), flat.reshape(1, -1))


def combine_kernel(onehot_ref, weight_ref, stream_ref, home_ref, out_ref):
    tokens = stream_ref.shape[0]
    picked = plain_dot(onehot_ref[...], home_ref[...])
    total = stream_ref[...]
    for k in range(weight_ref.shape[1]):
        total = total + picked[k * tokens : (k + 1) * tokens] * weight_ref[:, k : k + 1]
    out_ref[...] = total.astype(out_ref.dtype)


def combined(onehot, weight, stream, home):
    return pl.pallas_call(
        combine_kernel,
        out_shape=jax.ShapeDtypeStruct(stream.shape, jnp.bfloat16),
        in_specs=in_vmem(4),
        out_specs=in_vmem(1)[0],
        compiler_params=pltpu.CompilerParams(vmem_limit_bytes=12 << 20),
        cost_estimate=pl.CostEstimate(flops=100_000_000, bytes_accessed=1 << 20, transcendentals=0),
        name="combine_rows",
    )(onehot, weight, stream, home)


def hidden_rows(rows, gate, up):
    gated = plain_dot(rows, gate)
    return (gated * jax.nn.sigmoid(gated) * plain_dot(rows, up)).astype(jnp.bfloat16)


def first_kernel(rows, gate, up, down, out, gates, ups, downs, hidden, sems):
    width, width_ff = gate.shape
    cuts = [pl.ds(f, min(FF_TILE, width_ff - f)) for f in range(0, width_ff, FF_TILE)]
    wide_cuts = [pl.ds(f, 2 * FF_TILE) for f in range(0, width, 2 * FF_TILE)]
    copies = []
    for which, (source, here) in enumerate(((gate, gates), (up, ups), (down, downs))):
        places = wide_cuts if which == 2 else cuts
        copies.append(
            [
                pltpu.make_async_copy(source.at[:, p], here.at[:, p], sems.at[which, n])
                for n, p in enumerate(places)
            ]
        )
    for n in range(len(cuts)):
        copies[0][n].start()
        copies[1][n].start()
    for one in copies[2]:
        one.start()
    for n, p in enumerate(cuts):
        copies[0][n].wait()
        copies[1][n].wait()
        hidden[:, p] = hidden_rows(rows[...], gates[:, p], ups[:, p])
    for n, p in enumerate(wide_cuts):
        copies[2][n].wait()
        out[:, p] = plain_dot(hidden[...], downs[:, p]).astype(out.dtype)


def first_rows(rows, gate, up, down):
    count, width = rows.shape
    width_ff = gate.shape[1]
    shapes = [jax.ShapeDtypeStruct(a.shape, a.dtype) for a in (rows, gate, up, down)]
    return pl.pallas_call(
        first_kernel,
        out_shape=tuple(shapes),
        in_specs=[in_vmem(1)[0], *[pl.BlockSpec(memory_space=pltpu.HBM)] * 3],
        out_specs=tuple(in_vmem(4)),
        scratch_shapes=[
            pltpu.VMEM((count, width_ff), jnp.bfloat16),
            pltpu.SemaphoreType.DMA((3, 4)),
        ],
        compiler_params=pltpu.CompilerParams(vmem_limit_bytes=LIMIT_FIRST << 20),
        cost_estimate=pl.CostEstimate(
            flops=6 * count * width * width_ff, bytes_accessed=6 * width * width_ff, transcendentals=0
        ),
        name="first_rows",
    )(rows, gate, up, down)


def more_kernel(count, *refs):
    pieces, (gates, ups, downs), (out, hidden) = refs[:count], refs[count : count + 3], refs[count + 3 :]
    width, width_ff = gates.shape
    rows = pieces[0][...]
    if count > 1:
        rows = jnp.concatenate([piece[...] for piece in pieces], axis=0)
    for f in range(0, width_ff, FF_TILE):
        p = slice(f, min(f + FF_TILE, width_ff))
        hidden[:, p] = hidden_rows(rows, gates[:, p], ups[:, p])
    for f in range(0, width, 2 * FF_TILE):
        p = slice(f, f + 2 * FF_TILE)
        out[:, p] = plain_dot(hidden[...], downs[:, p]).astype(out.dtype)


def more_rows(pieces, weights):
    count, width = sum(piece.shape[0] for piece in pieces), pieces[0].shape[1]
    width_ff = weights[0].shape[1]
    return pl.pallas_call(
        partial(more_kernel, len(pieces)),
        out_shape=jax.ShapeDtypeStruct((count, width), jnp.bfloat16),
        in_specs=in_vmem(len(pieces) + 3),
        out_specs=in_vmem(1)[0],
        scratch_shapes=[pltpu.VMEM((count, width_ff), jnp.bfloat16)],
        compiler_params=pltpu.CompilerParams(vmem_limit_bytes=LIMIT_REST << 20),
        cost_estimate=pl.CostEstimate(
            flops=6 * count * width * width_ff, bytes_accessed=6 * width * width_ff, transcendentals=0
        ),
        name="more_rows",
    )(*pieces, *weights)


def body(
    receptance,
    head_keys,
    head_values,
    decay_logits,
    decay_boost,
    correction_logits,
    gate_logits,
    head_norm_gain,
    output_weight,
    residual,
    expert_norm_gain,
    routes,
    routing_weight,
    expert_gate_weight,
    expert_up_weight,
    expert_down_weight,
):
    outputs, whole = scanned(
        receptance, head_keys, head_values, decay_logits, decay_boost, correction_logits
    )
    weights = gathered_weight(output_weight)
    first, mine, swapped = incoming_state(whole)
    own, *blocks = finished(outputs, first, mine, swapped, gate_logits, head_norm_gain)
    rows_here = [shifted(b, "tp", k) for b, k in zip(blocks, OFFSETS)]
    sp_count = lax.axis_size(SP)
    tp_count = lax.axis_size("tp")
    capacity = max(2, 2 * TOK_DEV * TOP // (tp_count * sp_count))
    width_model = residual.shape[1]
    stream, outbound, onehot = projected(
        own,
        output_weight,
        rows_here,
        weights,
        residual,
        expert_norm_gain,
        routes,
        sp_count,
        capacity,
    )
    going = outbound.reshape(sp_count, 2 * capacity, width_model // 2)
    arrived = lax.all_to_all(going, SP, split_axis=0, concat_axis=0, tiled=True)
    arrived = arrived.reshape(-1, width_model)
    back, ahead = shifted(arrived, "tp", 1), shifted(arrived, "tp", -1)
    weights = (expert_gate_weight[0], expert_up_weight[0], expert_down_weight[0])
    own, *weights = first_rows(arrived, *weights)
    middle = arrived.shape[0] // 2
    away = [shifted(back[:middle], "tp", 1), shifted(ahead[middle:], "tp", -1)]
    back = more_rows([back], weights)
    ahead = more_rows([ahead], weights)
    away = more_rows(away, weights)
    parts = [own]
    for piece, k in ((back, -1), (ahead, 1), (away, 2)):
        parts.append(shifted(piece, "tp", k))
    total = sum(piece.astype(jnp.float32) for piece in parts).astype(jnp.bfloat16)
    total = total.reshape(sp_count, 2 * capacity, width_model // 2)
    home = lax.all_to_all(total, SP, split_axis=0, concat_axis=0, tiled=True)
    home = home.reshape(-1, width_model)
    return combined(onehot, routing_weight, stream, home)


def solution(mesh):
    torus = Mesh(
        mesh.devices.reshape(mesh.shape["grp"], 16, 2, mesh.shape["tp"]),
        ("grp", "sp_0", "sp_1", "tp"),
    )
    return jax.shard_map(
        body,
        mesh=torus,
        in_specs=(
            P(GRP_SP, "tp"),
            P(GRP_SP, "tp"),
            P(GRP_SP, "tp"),
            P(GRP_SP, "tp"),
            P(GRP_SP, "tp"),
            P(GRP_SP, "tp"),
            P(GRP_SP, "tp"),
            P("tp"),
            P("tp", None),
            P(GRP_SP_TP, None),
            P(),
            P(GRP_SP_TP, None),
            P(GRP_SP_TP, None),
            P(SP, None, "tp"),
            P(SP, None, "tp"),
            P(SP, "tp", None),
        ),
        out_specs=P(GRP_SP_TP, None),
        check_vma=False,
    )
```

```python
import math
from functools import partial

import jax
import jax.numpy as jnp
from jax import lax
from jax.experimental import pallas as pl
from jax.experimental.pallas import tpu as pltpu
from jax.sharding import Mesh
from jax.sharding import PartitionSpec as P


HEAD = 64
TOP = 2
BLK = 32
QUAD = 4
OFFSETS = (1, 3, 2)
FF_TILE = 256
LIMIT_FIRST = 42
LIMIT_REST = 18
HALF_DOWN = math.exp(-0.5)
TOK_DEV = 128
SP = ("sp_0", "sp_1")
GRP_SP = ("grp", "sp_0", "sp_1")
GRP_SP_TP = ("grp", "sp_0", "sp_1", "tp")


def shifted(x, axis, step):
    size = lax.axis_size(axis)
    return lax.ppermute(x, axis, [(i, (i + step) % size) for i in range(size)])


def within_quads(x, axis, step):
    size = lax.axis_size(axis)
    pairs = [(i, i // QUAD * QUAD + (i % QUAD + step) % QUAD) for i in range(size)]
    return lax.ppermute(x, axis, pairs)


def across_quads(x, axis, step):
    size = lax.axis_size(axis)
    return lax.ppermute(x, axis, [(i, i + step * QUAD) for i in range(size - step * QUAD)])


def chip_kernel(core_ref, own_ref, other_ref, chip_ref, sent_ref):
    core = core_ref[0]
    half = chip_ref.shape[0]
    for h in range(half):
        own = own_ref[core * half + h].astype(jnp.float32)
        other = other_ref[core * half + h].astype(jnp.float32)
        first = jnp.where(core == 0, own, other)
        second = jnp.where(core == 0, other, own)
        chip = joined(second, first)
        chip_ref[h] = chip
        sent_ref[h] = chip.astype(sent_ref.dtype)


def core_index():
    return lax.axis_index("sp_1").astype(jnp.int32).reshape(1)


def chip_map(own, other):
    shape = (own.shape[0] // 2, *own.shape[1:])
    return pl.pallas_call(
        chip_kernel,
        out_shape=(
            jax.ShapeDtypeStruct(shape, jnp.float32),
            jax.ShapeDtypeStruct(shape, jnp.bfloat16),
        ),
        in_specs=[pl.BlockSpec(memory_space=pltpu.SMEM), *in_vmem(2)],
        out_specs=tuple(in_vmem(2)),
        cost_estimate=pl.CostEstimate(flops=200_000_000, bytes_accessed=1 << 18, transcendentals=0),
        compiler_params=pltpu.CompilerParams(vmem_limit_bytes=8 << 20),
        name="chip_map",
    )(core_index(), own, other)


def joined(later, earlier):
    state = lax.broadcasted_iota(jnp.int32, later.shape, 1) >= HEAD
    return split_dot(later[:, :HEAD], earlier) + jnp.where(state, later, 0.0)


def quad_kernel(member_ref, chip_ref, *refs):
    *came, before_ref, sent_ref = refs
    member = member_ref[0]
    for h in range(chip_ref.shape[0]):
        pieces = [chip_ref[h]] + [piece[h].astype(jnp.float32) for piece in came]
        ordered = []
        for place in range(QUAD):
            piece = pieces[0]
            for k in range(1, QUAD):
                piece = jnp.where(member == (place + k) % QUAD, pieces[k], piece)
            ordered.append(piece)
        total = ordered[0]
        row = lax.broadcasted_iota(jnp.int32, total.shape, 0)
        col = lax.broadcasted_iota(jnp.int32, total.shape, 1)
        before = jnp.where(member == 0, (row == col).astype(jnp.float32), total)
        for place in range(1, QUAD):
            total = joined(ordered[place], total)
            if place < QUAD - 1:
                before = jnp.where(member == place + 1, total, before)
        before_ref[h] = before
        sent_ref[h] = total.astype(sent_ref.dtype)


def quad_map(chip, came):
    member = (lax.axis_index("sp_0") % QUAD).astype(jnp.int32).reshape(1)
    return pl.pallas_call(
        quad_kernel,
        out_shape=(
            jax.ShapeDtypeStruct(chip.shape, jnp.float32),
            jax.ShapeDtypeStruct(chip.shape, jnp.bfloat16),
        ),
        in_specs=[pl.BlockSpec(memory_space=pltpu.SMEM), *in_vmem(QUAD)],
        out_specs=tuple(in_vmem(2)),
        compiler_params=pltpu.CompilerParams(vmem_limit_bytes=8 << 20),
        cost_estimate=pl.CostEstimate(flops=200_000_000, bytes_accessed=1 << 18, transcendentals=0),
        name="quad_map",
    )(member, chip, *came)


def far_kernel(before_ref, *refs):
    *far, mine_ref = refs
    wide = jnp.float32
    for h in range(before_ref.shape[0]):
        reach = far[0][h][:, HEAD:].astype(wide)
        for piece in [*far[1:], before_ref]:
            later = piece[h].astype(wide)
            reach = split_dot(later[:, :HEAD], reach) + later[:, HEAD:]
        mine_ref[:, h * HEAD : (h + 1) * HEAD] = reach.astype(mine_ref.dtype)


def far_state(before, far):
    heads = before.shape[0]
    return pl.pallas_call(
        far_kernel,
        out_shape=jax.ShapeDtypeStruct((HEAD, heads * HEAD), jnp.bfloat16),
        in_specs=in_vmem(QUAD),
        out_specs=in_vmem(1)[0],
        compiler_params=pltpu.CompilerParams(vmem_limit_bytes=8 << 20),
        cost_estimate=pl.CostEstimate(flops=200_000_000, bytes_accessed=1 << 18, transcendentals=0),
        name="far_state",
    )(before, *far)


def incoming_state(packed):
    other = shifted(packed, "sp_1", 1)
    chip, sent = chip_map(packed, other)
    came = [within_quads(sent, "sp_0", k) for k in range(1, QUAD)]
    before, sent = quad_map(chip, came)
    far = [across_quads(sent, "sp_0", k) for k in range(QUAD - 1, 0, -1)]
    mine = far_state(before, far)
    swapped = shifted(mine, "sp_1", 1)
    return other, mine, swapped


def gathered_weight(weight):
    half = weight.shape[1] // 2
    core = lax.axis_index("sp_1")
    mine = lax.dynamic_slice_in_dim(weight, core * half, half, 1)
    mine = [shifted(mine, "tp", k) for k in OFFSETS]
    other = [shifted(piece, "sp_1", 1) for piece in mine]
    return mine, other


def split_dot(first, second):
    high_a, high_b = first.astype(jnp.bfloat16), second.astype(jnp.bfloat16)
    low_a = (first - high_a.astype(jnp.float32)).astype(jnp.bfloat16)
    low_b = (second - high_b.astype(jnp.float32)).astype(jnp.bfloat16)
    return plain_dot(high_a, high_b) + (plain_dot(high_a, low_b) + plain_dot(low_a, high_b))


def plain_dot(first, second, dims=((1,), (0,))):
    return lax.dot_general(
        first.astype(jnp.bfloat16),
        second.astype(jnp.bfloat16),
        (dims, ((), ())),
        preferred_element_type=jnp.float32,
    )


def scan_kernel(query_ref, key_ref, value_ref, decay_ref, boost_ref, rate_ref, out_ref, whole_ref):
    wide, narrow = jnp.float32, jnp.bfloat16
    length, width = key_ref.shape
    heads = width // HEAD
    blocks = length // BLK
    keyed = key_ref[...].astype(wide)
    query = query_ref[...].astype(wide)
    valued = value_ref[...]
    lane_r = lax.broadcasted_iota(jnp.int32, (width, width), 0) // HEAD
    lane_c = lax.broadcasted_iota(jnp.int32, (width, width), 1) // HEAD
    same_head = (lane_r == lane_c).astype(narrow)
    square = keyed * keyed
    square_high = square.astype(narrow)
    square_low = (square - square_high.astype(wide)).astype(narrow)
    norm = plain_dot(square_high, same_head) + plain_dot(square_low, same_head)
    unit = keyed * lax.rsqrt(norm + 1e-06)
    insert = unit * jax.nn.sigmoid(rate_ref[...].astype(wide))
    slow = jax.nn.sigmoid(decay_ref[...].astype(wide)) * HALF_DOWN
    log_decay = boost_ref[...] - slow
    row = lax.broadcasted_iota(jnp.int32, (length, length), 0)
    col = lax.broadcasted_iota(jnp.int32, (length, length), 1)
    same_block = row // BLK == col // BLK
    strict = same_block & (row > col)
    inclusive = same_block & (row >= col)
    sums = jnp.concatenate([inclusive.astype(narrow), same_block.astype(narrow)], axis=0)
    part, added = log_decay, 0.0
    for _ in range(3):
        piece = part.astype(narrow)
        added = added + plain_dot(sums, piece)
        part = part - piece.astype(wide)
    upto, final = added[:length], added[length:]
    remove_scaled = -unit * jnp.exp(upto - log_decay)
    query_scaled = query * jnp.exp(upto)
    shrink = jnp.exp(-upto)
    insert_scaled = (insert * shrink).astype(narrow)
    key_scaled = (keyed * shrink).astype(narrow)
    tail = jnp.exp(final - upto)
    insert_tail = (insert * tail).astype(narrow)
    key_tail = (keyed * tail).astype(narrow)
    kept = jnp.exp(final)
    every = range(heads)
    lanes = [slice(h * HEAD, (h + 1) * HEAD) for h in every]
    pair = [
        plain_dot(
            jnp.concatenate([remove_scaled[:, lanes[h]], query_scaled[:, lanes[h]]], axis=0),
            jnp.concatenate([insert_scaled[:, lanes[h]], key_scaled[:, lanes[h]]], axis=0),
            ((1,), (1,)),
        )
        for h in every
    ]
    among = [jnp.where(strict, pair[h][:length, :length], 0.0).astype(narrow) for h in every]
    read = [jnp.where(inclusive, pair[h][length:, :length], 0.0).astype(narrow) for h in every]
    by_keys = [
        jnp.concatenate(
            [
                jnp.where(strict, pair[h][:length, length:], 0.0),
                jnp.where(inclusive, pair[h][length:, length:], 0.0),
            ],
            axis=0,
        ).astype(narrow)
        for h in every
    ]
    from_values = [plain_dot(by_keys[h], valued[:, lanes[h]]) for h in every]
    solved = [
        jnp.concatenate([remove_scaled[:, lanes[h]], from_values[h][:length]], axis=1)
        for h in every
    ]
    power = among
    covered = 1
    while covered < BLK:
        solved = [solved[h] + plain_dot(power[h], solved[h]) for h in every]
        covered = 2 * covered
        if covered < BLK:
            power = [plain_dot(power[h], power[h]).astype(narrow) for h in every]
    reading = [
        jnp.concatenate([query_scaled[:, lanes[h]], from_values[h][length:]], axis=1)
        + plain_dot(read[h], solved[h])
        for h in every
    ]
    wide_r = lax.broadcasted_iota(jnp.int32, (HEAD, 2 * HEAD), 0)
    wide_c = lax.broadcasted_iota(jnp.int32, (HEAD, 2 * HEAD), 1)
    diagonal = wide_r == wide_c
    is_state = wide_c >= HEAD
    none = jnp.zeros((BLK, HEAD), narrow)
    so_far = [None] * heads
    for n in range(blocks):
        rows = slice(n * BLK, (n + 1) * BLK)
        maps = []
        for h in every:
            sources = jnp.concatenate([insert_tail[rows, lanes[h]], key_tail[rows, lanes[h]]], axis=0)
            targets = jnp.concatenate(
                [
                    solved[h][rows].astype(narrow),
                    jnp.concatenate([none, valued[rows, lanes[h]]], axis=1),
                ],
                axis=0,
            )
            keeps = kept[n * BLK : n * BLK + 1, lanes[h]]
            keeps = jnp.concatenate([keeps, keeps], axis=1)
            maps.append(
                plain_dot(sources, targets, ((0,), (0,))) + jnp.where(diagonal, keeps, 0.0)
            )
        for h in every:
            here = reading[h][rows]
            if n == 0:
                out_ref[h, rows, :] = here
                so_far[h] = maps[h]
            else:
                moved = split_dot(here[:, :HEAD], so_far[h])
                local = lax.broadcasted_iota(jnp.int32, here.shape, 1) >= HEAD
                out_ref[h, rows, :] = moved + jnp.where(local, here, 0.0)
                so_far[h] = split_dot(maps[h][:, :HEAD], so_far[h]) + jnp.where(
                    is_state, maps[h], 0.0
                )
    for h in every:
        whole_ref[h] = so_far[h].astype(narrow)


def in_vmem(count):
    return [pl.BlockSpec(memory_space=pltpu.VMEM)] * count


def scanned(*arrays):
    length, width = arrays[0].shape
    heads = width // HEAD
    return pl.pallas_call(
        scan_kernel,
        out_shape=(
            jax.ShapeDtypeStruct((heads, length, 2 * HEAD), jnp.float32),
            jax.ShapeDtypeStruct((heads, HEAD, 2 * HEAD), jnp.bfloat16),
        ),
        in_specs=in_vmem(6),
        out_specs=tuple(in_vmem(2)),
        cost_estimate=pl.CostEstimate(flops=4_000_000_000, bytes_accessed=1 << 20, transcendentals=0),
        name="scan_blocks",
    )(*arrays)


def finish_kernel(
    place_ref, out_ref, first_ref, mine_ref, swapped_ref, gate_ref, gain_ref, *refs
):
    *blocks, gated_ref = refs
    wide = jnp.float32
    heads = out_ref.shape[0]
    later_core = place_ref[0] > 0
    mine, swapped = mine_ref[...].astype(wide), swapped_ref[...].astype(wide)
    low = jnp.where(later_core, swapped, mine)
    high = jnp.where(later_core, mine, swapped)
    parts = []
    for h in range(heads):
        before = first_ref[h].astype(wide)
        reach = (low, high)[h // 2][:, h % 2 * HEAD : (h % 2 + 1) * HEAD]
        passed = split_dot(before[:, :HEAD], reach) + before[:, HEAD:]
        reach = jnp.where(later_core, passed, reach)
        here = out_ref[h]
        mixed = split_dot(here[:, :HEAD], reach) + here[:, HEAD:]
        centre = mixed - jnp.mean(mixed, axis=1, keepdims=True)
        spread = jnp.mean(centre * centre, axis=1, keepdims=True)
        parts.append(centre * lax.rsqrt(spread + 0.00064))
    normed = jnp.concatenate(parts, axis=1) * gain_ref[...]
    gated_ref[...] = normed * jax.nn.sigmoid(gate_ref[...].astype(wide))
    count = blocks[0].shape[0]
    for block, k in zip(blocks, (0, *OFFSETS)):
        start = (place_ref[1] + k) % len(blocks) * count
        block[...] = gated_ref[pl.ds(pl.multiple_of(start, count), count), :].astype(block.dtype)


def finished(outputs, first, mine, swapped, gate_logits, gain):
    count = lax.axis_size("tp")
    rows, width = gate_logits.shape
    place = jnp.stack([lax.axis_index("sp_1"), lax.axis_index("tp")]).astype(jnp.int32)
    block = jax.ShapeDtypeStruct((rows // count, width), jnp.bfloat16)
    return pl.pallas_call(
        finish_kernel,
        out_shape=(block,) * count,
        in_specs=[pl.BlockSpec(memory_space=pltpu.SMEM), *in_vmem(6)],
        out_specs=tuple(in_vmem(count)),
        scratch_shapes=[pltpu.VMEM((rows, width), jnp.float32)],
        cost_estimate=pl.CostEstimate(flops=400_000_000, bytes_accessed=1 << 19, transcendentals=0),
        compiler_params=pltpu.CompilerParams(vmem_limit_bytes=12 << 20),
        name="finish_heads",
    )(place, outputs, first, mine, swapped, gate_logits, gain.reshape(1, -1))


def project_kernel(count, core_ref, own_ref, weight_ref, *refs):
    rows, mine, other = refs[:count], refs[count : 2 * count], refs[2 * count : 3 * count]
    residual_ref, gain_ref, placed_ref, stream_ref, out_ref = refs[3 * count :]
    halves = []
    for side in (mine, other):
        halves.append(sum(plain_dot(r[...], w[...]) for r, w in zip(rows, side)))
    swap = core_ref[0] > 0
    left = jnp.where(swap, halves[1], halves[0])
    right = jnp.where(swap, halves[0], halves[1])
    branch = plain_dot(own_ref[...], weight_ref[...]) + jnp.concatenate([left, right], axis=1)
    stream = residual_ref[...].astype(jnp.float32) + branch
    stream_ref[...] = stream
    scale = lax.rsqrt(jnp.mean(stream * stream, axis=1, keepdims=True) + 1e-06)
    normal = (stream * scale * gain_ref[...]).astype(jnp.bfloat16)
    out_ref[...] = plain_dot(placed_ref[...], normal, ((0,), (0,))).astype(out_ref.dtype)


def projected(own, weight, rows, weights, residual, gain, placed):
    count, width = len(rows), residual.shape[1]
    return pl.pallas_call(
        partial(project_kernel, count),
        out_shape=(
            jax.ShapeDtypeStruct(residual.shape, jnp.float32),
            jax.ShapeDtypeStruct((placed.shape[1], width), jnp.bfloat16),
        ),
        in_specs=[pl.BlockSpec(memory_space=pltpu.SMEM), *in_vmem(3 * count + 5)],
        out_specs=tuple(in_vmem(2)),
        cost_estimate=pl.CostEstimate(flops=800_000_000, bytes_accessed=5 << 20, transcendentals=0),
        compiler_params=pltpu.CompilerParams(vmem_limit_bytes=20 << 20),
        name="project_rows",
    )(core_index(), own, weight, *rows, *weights[0], *weights[1], residual, gain.reshape(1, -1), placed)


def hidden_rows(rows, gate, up):
    gated = plain_dot(rows, gate)
    return (gated * jax.nn.sigmoid(gated) * plain_dot(rows, up)).astype(jnp.bfloat16)


def first_kernel(rows, gate, up, down, out, gates, ups, downs, hidden, sems):
    width, width_ff = gate.shape
    cuts = [pl.ds(f, min(FF_TILE, width_ff - f)) for f in range(0, width_ff, FF_TILE)]
    wide_cuts = [pl.ds(f, 2 * FF_TILE) for f in range(0, width, 2 * FF_TILE)]
    copies = []
    for which, (source, here) in enumerate(((gate, gates), (up, ups), (down, downs))):
        places = wide_cuts if which == 2 else cuts
        copies.append(
            [
                pltpu.make_async_copy(source.at[:, p], here.at[:, p], sems.at[which, n])
                for n, p in enumerate(places)
            ]
        )
    for n in range(len(cuts)):
        copies[0][n].start()
        copies[1][n].start()
    for one in copies[2]:
        one.start()
    for n, p in enumerate(cuts):
        copies[0][n].wait()
        copies[1][n].wait()
        hidden[:, p] = hidden_rows(rows[...], gates[:, p], ups[:, p])
    for n, p in enumerate(wide_cuts):
        copies[2][n].wait()
        out[:, p] = plain_dot(hidden[...], downs[:, p]).astype(out.dtype)


def first_rows(rows, gate, up, down):
    count, width = rows.shape
    width_ff = gate.shape[1]
    shapes = [jax.ShapeDtypeStruct(a.shape, a.dtype) for a in (rows, gate, up, down)]
    return pl.pallas_call(
        first_kernel,
        out_shape=tuple(shapes),
        in_specs=[in_vmem(1)[0], *[pl.BlockSpec(memory_space=pltpu.HBM)] * 3],
        out_specs=tuple(in_vmem(4)),
        scratch_shapes=[
            pltpu.VMEM((count, width_ff), jnp.bfloat16),
            pltpu.SemaphoreType.DMA((3, 4)),
        ],
        compiler_params=pltpu.CompilerParams(vmem_limit_bytes=LIMIT_FIRST << 20),
        cost_estimate=pl.CostEstimate(
            flops=6 * count * width * width_ff, bytes_accessed=6 * width * width_ff, transcendentals=0
        ),
        name="first_rows",
    )(rows, gate, up, down)


def more_kernel(count, *refs):
    pieces, (gates, ups, downs), (out, hidden) = refs[:count], refs[count : count + 3], refs[count + 3 :]
    width, width_ff = gates.shape
    rows = pieces[0][...]
    if count > 1:
        rows = jnp.concatenate([piece[...] for piece in pieces], axis=0)
    for f in range(0, width_ff, FF_TILE):
        p = slice(f, min(f + FF_TILE, width_ff))
        hidden[:, p] = hidden_rows(rows, gates[:, p], ups[:, p])
    for f in range(0, width, 2 * FF_TILE):
        p = slice(f, f + 2 * FF_TILE)
        out[:, p] = plain_dot(hidden[...], downs[:, p]).astype(out.dtype)


def more_rows(pieces, weights):
    count, width = sum(piece.shape[0] for piece in pieces), pieces[0].shape[1]
    width_ff = weights[0].shape[1]
    return pl.pallas_call(
        partial(more_kernel, len(pieces)),
        out_shape=jax.ShapeDtypeStruct((count, width), jnp.bfloat16),
        in_specs=in_vmem(len(pieces) + 3),
        out_specs=in_vmem(1)[0],
        scratch_shapes=[pltpu.VMEM((count, width_ff), jnp.bfloat16)],
        compiler_params=pltpu.CompilerParams(vmem_limit_bytes=LIMIT_REST << 20),
        cost_estimate=pl.CostEstimate(
            flops=6 * count * width * width_ff, bytes_accessed=6 * width * width_ff, transcendentals=0
        ),
        name="more_rows",
    )(*pieces, *weights)


def body(
    receptance,
    head_keys,
    head_values,
    decay_logits,
    decay_boost,
    correction_logits,
    gate_logits,
    head_norm_gain,
    output_weight,
    residual,
    expert_norm_gain,
    routes,
    routing_weight,
    expert_gate_weight,
    expert_up_weight,
    expert_down_weight,
):
    outputs, whole = scanned(
        receptance, head_keys, head_values, decay_logits, decay_boost, correction_logits
    )
    weights = gathered_weight(output_weight)
    first, mine, swapped = incoming_state(whole)
    own, *blocks = finished(outputs, first, mine, swapped, gate_logits, head_norm_gain)
    rows_here = [shifted(b, "tp", k) for b, k in zip(blocks, OFFSETS)]
    sp_count = lax.axis_size(SP)
    tp_count = lax.axis_size("tp")
    capacity = max(2, 2 * TOK_DEV * TOP // (tp_count * sp_count))
    local_count, width_model = residual.shape
    flat_routes = routes.reshape(-1)
    expert_ids = jnp.arange(sp_count, dtype=jnp.int32)
    chosen = (flat_routes[:, None] == expert_ids[None, :]).astype(jnp.int32)
    earlier = jnp.cumsum(chosen, axis=0) - chosen
    rank = jnp.sum(earlier * chosen, axis=1)
    place = flat_routes * capacity + rank
    places = jnp.arange(sp_count * capacity, dtype=jnp.int32)
    onehot = (place[:, None] == places[None, :]).astype(jnp.bfloat16)
    placed = jnp.sum(onehot.reshape(local_count, TOP, sp_count * capacity), axis=1)
    placed, onehot, routing_weight = lax.optimization_barrier((placed, onehot, routing_weight))
    stream, outbound = projected(
        own, output_weight, rows_here, weights, residual, expert_norm_gain, placed
    )
    going = outbound.reshape(sp_count, 2 * capacity, width_model // 2)
    arrived = lax.all_to_all(going, SP, split_axis=0, concat_axis=0, tiled=True)
    arrived = arrived.reshape(-1, width_model)
    back, ahead = shifted(arrived, "tp", 1), shifted(arrived, "tp", -1)
    weights = (expert_gate_weight[0], expert_up_weight[0], expert_down_weight[0])
    own, *weights = first_rows(arrived, *weights)
    middle = arrived.shape[0] // 2
    away = [shifted(back[:middle], "tp", 1), shifted(ahead[middle:], "tp", -1)]
    back = more_rows([back], weights)
    ahead = more_rows([ahead], weights)
    away = more_rows(away, weights)
    parts = [own]
    for piece, k in ((back, -1), (ahead, 1), (away, 2)):
        parts.append(shifted(piece, "tp", k))
    total = sum(piece.astype(jnp.float32) for piece in parts).astype(jnp.bfloat16)
    total = total.reshape(sp_count, 2 * capacity, width_model // 2)
    home = lax.all_to_all(total, SP, split_axis=0, concat_axis=0, tiled=True)
    home = home.reshape(-1, width_model)
    picked = jnp.dot(onehot, home, preferred_element_type=jnp.float32)
    routed = jnp.sum(
        picked.reshape(local_count, TOP, width_model) * routing_weight[:, :, None], axis=1
    )
    return (stream + routed).astype(jnp.bfloat16)


def solution(mesh):
    torus = Mesh(
        mesh.devices.reshape(mesh.shape["grp"], 16, 2, mesh.shape["tp"]),
        ("grp", "sp_0", "sp_1", "tp"),
    )
    return jax.shard_map(
        body,
        mesh=torus,
        in_specs=(
            P(GRP_SP, "tp"),
            P(GRP_SP, "tp"),
            P(GRP_SP, "tp"),
            P(GRP_SP, "tp"),
            P(GRP_SP, "tp"),
            P(GRP_SP, "tp"),
            P(GRP_SP, "tp"),
            P("tp"),
            P("tp", None),
            P(GRP_SP_TP, None),
            P(),
            P(GRP_SP_TP, None),
            P(GRP_SP_TP, None),
            P(SP, None, "tp"),
            P(SP, None, "tp"),
            P(SP, "tp", None),
        ),
        out_specs=P(GRP_SP_TP, None),
        check_vma=False,
    )
```
